32 devices in a mesh: ep: 8 (over z, x), tp: 4 (over y, core).
Axes of the slice: x: 2, y: 2, z: 4, core: 2. Of those that a mesh axis runs over, the one named last changes fastest.
Arguments:
- queries: bfloat16 [2048, 8, 128], P('ep', 'tp'), may hold values from -256 to 256
- keys: bfloat16 [2048, 4, 128], P('ep', 'tp'), may hold values from -8 to 8
- values: bfloat16 [2048, 4, 128], P('ep', 'tp'), may hold values from -6 to 6
- attn_lambda: float32 [8], P('tp'), may hold values from 0.3 to 0.8
- head_gain: float32 [128], replicated, may hold values from 0.1 to 1.9
- w_out: bfloat16 [1024, 2048], replicated, may hold values from -0.1875 to 0.1875
- moe_rows: bfloat16 [4096, 2048], P('ep'), may hold values from -6 to 6
- moe_gain: float32 [2048], replicated, may hold values from 0.1 to 1.9
- routes: int32 [4096, 2], P('ep'), may hold values from 0 to 7, all different within a row; in each aligned block of 128 rows (0 to 127, 128 to 255, ...) at most 64 rows name the same one
- route_weights: float32 [4096, 2], P('ep'), may hold values from 0.1 to 1
- w_gate: bfloat16 [8, 2048, 1024], P('ep', None, 'tp'), may hold values from -0.125 to 0.125
- w_up: bfloat16 [8, 2048, 1024], P('ep', None, 'tp'), may hold values from -0.125 to 0.125
- w_down: bfloat16 [8, 1024, 2048], P('ep', 'tp'), may hold values from -0.1875 to 0.1875
Outputs:
- mixer_out: bfloat16 [2048, 2048], P(('ep', 'tp'))
- moe_out: bfloat16 [4096, 2048], P(('ep', 'tp'))
The draws below stay inside these ranges and needn't reach their ends.
Inputs may be any that keep to these rules, and one draw needn't show every extreme that they name: `routes`: each row names 2 different experts. In each aligned block of 128 rows (the rows of moe_out that one device holds) no expert is named by more than 64 rows, a bound that some block reaches.
All inputs are finite; a program needn't handle non-finite values.
Results may differ from the reference program's by a relative error of at most 0.011.
Values may be sent and summed in bfloat16 or wider, within the bound.
A program may use at most 128 MiB of HBM per device.

```python
import math
import jax
import jax.numpy as jnp
import numpy as np
from jax import lax

D = 2048
HQ = 8
KVH = 4
HEAD = 64
VDIM = 128
FF = 1024
TOPK = 2
MOE_DEV = 128
EXPERTS = 8
CAP = 64
ATT_TOKENS = 2048
MOE_TOKENS = 4096
N_EP = 8
N_TP = 4


def pair_draw(key):
    spread = 1.75 ** 0.5
    base_q = jax.random.truncated_normal(jax.random.fold_in(key, 101), -4.5, 4.5, (ATT_TOKENS, HQ, 2, HEAD), jnp.float32) * spread
    base_k = jax.random.truncated_normal(jax.random.fold_in(key, 102), -4.5, 4.5, (ATT_TOKENS, KVH, 2, HEAD), jnp.float32) * spread
    return (base_q.reshape(ATT_TOKENS, HQ, 2 * HEAD), base_k.reshape(ATT_TOKENS, KVH, 2 * HEAD))


def draw_queries(key, part):
    return pair_draw(key)[0].astype(jnp.bfloat16)


def draw_keys(key, part):
    return pair_draw(key)[1].astype(jnp.bfloat16)


def steps_of(key, shape, shards, low, high):
    factor_of = 1.0
    for dim, blocks in shards:
        steps = jax.random.uniform(jax.random.fold_in(jax.random.fold_in(key, 6), dim), (blocks,), jnp.float32, low / len(shards), high / len(shards))
        factor_of = factor_of * jnp.repeat(jnp.exp(steps), shape[dim] // blocks).reshape((-1,) + (1,) * (len(shape) - 1 - dim))
    return factor_of


def deal_out(key, own, number, rows, number_of, top, limit, slope):
    order = jax.random.permutation(key, number_of)
    heavy_load, ordinary = load_shares(number_of, rows * top, limit, slope, True), load_shares(number_of, rows * top, limit, slope, False)
    places = jnp.arange(number_of)

    def named(tallies, offset_by):
        used = int((tallies > 0).sum())
        fixed = max(1, used // 4)
        moved = fixed + (places - fixed + offset_by * (used - fixed)) % max(1, number_of - fixed)
        return jnp.zeros((number_of,), jnp.int32).at[order[jnp.where(places < fixed, places, moved)]].set(jnp.asarray(tallies, jnp.int32))

    tallies = jnp.where(number % 4 == 0, named(heavy_load, number // 4), named(ordinary, number - number // 4 - 1))
    mixed = jax.random.permutation(jax.random.fold_in(own, 3), number_of)
    source_of, taker = mixed[0:number_of // 2 * 2:2], mixed[1:number_of // 2 * 2:2]
    slack = jnp.minimum(tallies[source_of] - 1, limit - tallies[taker]) // 2
    slack = jnp.where((source_of == order[0]) | (taker == order[0]) | (tallies[taker] == 0), 0, jnp.maximum(slack, 0))
    moved = jax.random.randint(jax.random.fold_in(own, 4), (number_of // 2,), 0, 1 << 20) % (slack + 1)
    tallies = tallies.at[source_of].add(-moved).at[taker].add(moved)
    members = jnp.searchsorted(jnp.cumsum(tallies), jnp.arange(rows * top), side="right").astype(jnp.int32)
    table = members.reshape(top, rows).T
    table = table[jax.random.permutation(jax.random.fold_in(own, 1), rows)]
    offset_by = jax.random.randint(jax.random.fold_in(own, 2), (rows, 1), 0, top)
    return jnp.take_along_axis(table, (jnp.arange(top)[None, :] + offset_by) % top, axis=1)


def load_shares(amount, total, bound, lean, full):
    weights = [(1 << 20) // math.isqrt(standing ** lean) + 1 for standing in range(1, amount + 1)]
    largest = bound if full else min(bound, max(-(-total // amount), total * weights[0] // sum(weights)))
    least = 1 if total - largest >= amount - 1 else 0
    counts, spare = [largest] + [least] * (amount - 1), total - largest - least * (amount - 1)
    while spare > 0:
        free = [i for i in range(1, amount) if counts[i] < largest] or [i for i in range(1, amount) if counts[i] < bound]
        pool, budget = sum([weights[i] for i in free]), spare
        for i in free:
            extra = min(bound - counts[i], max(1, budget * weights[i] // pool), spare)
            counts[i] = counts[i] + extra
            spare = spare - extra
    return np.array(counts)


def normal_values(rng, extent, deviation, limit, split=(), kind=jnp.bfloat16):
    entries = deviation * jax.random.normal(rng, extent, jnp.float32)
    if split:
        entries = entries * steps_of(rng, extent, split, -0.22, 0.18)
    return jnp.clip(entries, -limit, limit).astype(kind)


def setup_inputs(seed: int = 0) -> dict:
    streams_of = jax.random.split(jax.random.key(seed), 14)
    queries = draw_queries(jax.random.fold_in(streams_of[13], 71), 0)
    keys = draw_keys(jax.random.fold_in(streams_of[13], 71), 0)
    values = normal_values(streams_of[2], (ATT_TOKENS, KVH, VDIM), 1.0, 6.0, ((0, 8), (1, 4)))
    attn_lambda = jnp.clip(0.3 + 0.5 * jax.random.uniform(streams_of[3], (HQ,), jnp.float32) ** steps_of(streams_of[3], (HQ,), ((0, 4),), -0.2, 0.2), 0.3, 0.8)
    head_gain = jnp.clip(1.0 + 0.18 * jax.random.normal(streams_of[4], (VDIM,), jnp.float32), 0.1, 1.9)
    w_out = normal_values(streams_of[5], (HQ * VDIM, D), (HQ * VDIM) ** -0.5, 0.1875)
    moe_rows = normal_values(streams_of[6], (MOE_TOKENS, D), 1.0, 6.0, ((0, 8),))
    moe_gain = jnp.clip(1.0 + 0.18 * jax.random.normal(streams_of[7], (D,), jnp.float32), 0.1, 1.9)
    routes_keys = jax.random.split(jax.random.fold_in(streams_of[8], 1), MOE_TOKENS // MOE_DEV)
    routes_turns = jax.random.permutation(jax.random.fold_in(streams_of[8], 3), MOE_TOKENS // MOE_DEV)
    routes = jax.vmap(lambda own, number: deal_out(jax.random.fold_in(streams_of[8], 2), own, number, MOE_DEV, EXPERTS, TOPK, CAP, 1))(routes_keys, routes_turns).reshape((MOE_TOKENS, TOPK))
    route_weights = jnp.clip(0.1 + 0.9 * jax.random.uniform(streams_of[9], (MOE_TOKENS, TOPK), jnp.float32) ** steps_of(streams_of[9], (MOE_TOKENS, TOPK), ((0, 8),), -0.2, 0.2), 0.1, 1.0)
    w_gate = normal_values(streams_of[10], (EXPERTS, D, FF), D ** -0.5, 0.125, ((0, 8), (2, 4)))
    w_up = normal_values(streams_of[11], (EXPERTS, D, FF), D ** -0.5, 0.125, ((0, 8), (2, 4)))
    w_down = normal_values(streams_of[12], (EXPERTS, FF, D), FF ** -0.5, 0.1875, ((0, 8), (1, 4)))
    return dict(queries=queries, keys=keys, values=values, attn_lambda=attn_lambda, head_gain=head_gain, w_out=w_out, moe_rows=moe_rows, moe_gain=moe_gain, routes=routes, route_weights=route_weights, w_gate=w_gate, w_up=w_up, w_down=w_down)


EPSILON = 1e-06
MASKED = -1e+30

def reference(queries, keys, values, attn_lambda, head_gain, w_out, moe_rows, moe_gain, routes, route_weights, w_gate, w_up, w_down):
    length = queries.shape[0]
    per_key = HQ // KVH
    key_all = jnp.repeat(keys.astype(jnp.float32).reshape(length, KVH, 2, HEAD), per_key, axis=1)
    value_all = jnp.repeat(values.astype(jnp.float32), per_key, axis=1)
    block_len = math.gcd(length, 256)
    block_count = length // block_len
    query_all = queries.astype(jnp.float32).reshape(block_count, block_len, HQ, 2, HEAD)
    key_pos = jnp.arange(length, dtype=jnp.int32)

    def one_block(inputs):
        query_blk, block_index = inputs
        query_pos = block_index * block_len + jnp.arange(block_len, dtype=jnp.int32)
        scores = jnp.einsum('qhmd,khmd->hmqk', query_blk, key_all) * HEAD ** (-0.5)
        allowed = key_pos[None, :] <= query_pos[:, None]
        scores = jnp.where(allowed, scores, MASKED)
        row_max = lax.optimization_barrier(jnp.max(scores, axis=-1, keepdims=True))
        weights = jnp.exp(scores - row_max)
        totals = lax.optimization_barrier(jnp.sum(weights, axis=-1))
        rounded = lax.optimization_barrier(weights.astype(jnp.bfloat16)).astype(jnp.float32)
        numerator = jnp.einsum('hmqk,khv->hmqv', rounded, value_all)
        ratios = numerator / totals[..., None]
        head_out = ratios[:, 0] - attn_lambda[:, None, None] * ratios[:, 1]
        inv_rms = lax.rsqrt(lax.optimization_barrier(jnp.mean(head_out * head_out, axis=-1, keepdims=True)) + EPSILON)
        normed_heads = (head_out * inv_rms * head_gain).astype(jnp.bfloat16)
        return jnp.transpose(normed_heads, (1, 0, 2)).reshape(block_len, HQ * VDIM)
    attn_rows = lax.map(one_block, (query_all, jnp.arange(block_count, dtype=jnp.int32)))
    attn_rows = attn_rows.reshape(length, HQ * VDIM)
    mixer_out = jnp.dot(attn_rows, w_out, preferred_element_type=jnp.float32).astype(jnp.bfloat16)
    rows_f = moe_rows.astype(jnp.float32)
    normed = (rows_f * lax.rsqrt(lax.optimization_barrier(jnp.mean(rows_f * rows_f, axis=-1, keepdims=True)) + EPSILON) * moe_gain).astype(jnp.bfloat16)
    tokens = moe_rows.shape[0]
    pairs = tokens * TOPK
    flat_ids = routes.reshape(-1).astype(jnp.int32)
    matches = (flat_ids[:, None] == jnp.arange(EXPERTS, dtype=jnp.int32)[None, :]).astype(jnp.int32)
    earlier = jnp.cumsum(matches, axis=0) - matches
    position = lax.optimization_barrier(jnp.sum(earlier * matches, axis=1)).astype(jnp.int32)
    slot_total = N_EP * N_TP * CAP
    pair_table = jnp.full((EXPERTS, slot_total), pairs, dtype=jnp.int32)
    pair_table = pair_table.at[flat_ids, position].set(jnp.arange(pairs, dtype=jnp.int32))
    token_table = jnp.where(pair_table < pairs, pair_table // TOPK, tokens).astype(jnp.int32)
    weight_flat = jnp.concatenate([route_weights.reshape(-1), jnp.zeros((1,), jnp.float32)])
    weight_table = weight_flat[pair_table]
    padded = jnp.concatenate([normed, jnp.zeros((1, D), jnp.bfloat16)], axis=0)
    group_width = FF // N_TP

    def one_expert(accumulated, inputs):
        token_row, weight_row, gate_w, up_w, down_w = inputs
        chosen = padded[token_row]
        gate_out = jnp.dot(chosen, gate_w, preferred_element_type=jnp.float32)
        up_out = jnp.dot(chosen, up_w, preferred_element_type=jnp.float32)
        hidden = (jax.nn.silu(gate_out) * up_out).astype(jnp.bfloat16)
        partials = jnp.einsum('stf,tfd->tsd', hidden.reshape(slot_total, N_TP, group_width).astype(jnp.float32), down_w.reshape(N_TP, group_width, D).astype(jnp.float32))
        partials = lax.optimization_barrier(partials.astype(jnp.bfloat16)).astype(jnp.float32)
        expert_out = lax.optimization_barrier(lax.optimization_barrier(jnp.sum(partials, axis=0)).astype(jnp.bfloat16)).astype(jnp.float32)
        accumulated = accumulated.at[token_row].add(weight_row[:, None] * expert_out)
        return (accumulated, None)
    start_total = jnp.zeros((tokens + 1, D), jnp.float32)
    accumulated, unused = lax.scan(one_expert, start_total, (token_table, weight_table, w_gate, w_up, w_down))
    moe_out = accumulated[:tokens].astype(jnp.bfloat16)
    return (mixer_out, moe_out)
```

```python
import functools

import jax
import jax.numpy as jnp
from jax import lax
from jax.experimental import pallas as pl
from jax.experimental.pallas import tpu as pltpu
from jax.sharding import PartitionSpec as P

EPSILON = 1e-06
MASKED = -1e30


def rms_scaled(values_f, gain):
    mean_sq = jnp.mean(values_f * values_f, axis=-1, keepdims=True)
    return values_f * lax.rsqrt(mean_sq + EPSILON) * gain


def expert_kernel(
    n,
    out_ref,
    near_ref,
    mine_ref,
    kv_ref,
    gate_ref,
    up_ref,
    down_ref,
    mix_ref,
    res_ref,
    kv_out,
    slots,
    part,
    pair_in,
    col_in,
    back,
    hidden_ref,
    acc,
    send_k,
    recv_k,
    send_a,
    recv_a,
    send_y,
    recv_y,
    send_c,
    recv_c,
    send_b,
    recv_b,
    send_p,
    recv_p,
    send_q,
    recv_q,
    send_r,
    recv_r,
    local_sem,
):
    me = lax.axis_index("ep")
    tp = lax.axis_index("tp")
    row = tp // 2
    col = tp % 2
    other_row = 1 - row
    other_col = 1 - col
    pair_peer = row * 2 + other_col
    row_peer = other_row * 2 + col
    own_blk = col * 2 + row
    far_blk = col * 2 + other_row
    slot_count = slots.shape[2]
    width = slots.shape[3]

    near = near_ref.shape[0]
    bits = [1 << b for b in range(n.bit_length() - 1)]

    def partner(d):
        total = 0
        for bit in bits:
            total = total + (me // bit + d // bit) % 2 * bit
        return total

    def remote(src, dst, ssem, rsem, ep_id, tp_id):
        return pltpu.make_async_remote_copy(
            src_ref=src,
            dst_ref=dst,
            send_sem=ssem,
            recv_sem=rsem,
            device_id=(ep_id, tp_id),
            device_id_type=pl.DeviceIdType.MESH,
        )

    barrier = pltpu.get_barrier_semaphore()

    @pl.loop(1, n)
    def _(d):
        pl.semaphore_signal(
            barrier, inc=1, device_id=(partner(d), tp), device_id_type=pl.DeviceIdType.MESH
        )

    for peer in (pair_peer, row_peer):
        pl.semaphore_signal(
            barrier, inc=1, device_id=(me, peer), device_id_type=pl.DeviceIdType.MESH
        )
    keep = pltpu.make_async_copy(kv_ref, kv_out.at[me], local_sem.at[4])
    keep.start()
    fills = [
        pltpu.make_async_copy(
            mine_ref.at[b], slots.at[0, (b % 2) * 2 + b // 2], local_sem.at[b]
        )
        for b in range(4)
    ]
    for fill in fills:
        fill.start()
    pl.semaphore_wait(barrier, n + 1)

    def copy_a(d):
        return remote(
            out_ref.at[d], slots.at[d, own_blk], send_a.at[d], recv_a.at[d], partner(d), tp
        )

    def copy_k(d):
        return remote(kv_ref, kv_out.at[me], send_k.at[d], recv_k.at[d], partner(d), tp)

    def copy_f(d):
        block = kv_out.at[partner(near)]
        return remote(block, block, send_k.at[d], recv_k.at[d], partner(d - near), tp)

    def copy_n(d):
        return remote(
            near_ref.at[d], slots.at[d, far_blk], send_y.at[d], recv_y.at[d], partner(d), tp
        )

    def copy_y(d):
        block = slots.at[d, own_blk]
        return remote(block, block, send_y.at[d], recv_y.at[d], me, row_peer)

    def copy_c(d):
        block = slots.at[d, own_blk]
        return remote(block, block, send_c.at[d], recv_c.at[d], me, pair_peer)

    def copy_b(d):
        block = slots.at[d, far_blk]
        return remote(block, block, send_b.at[d], recv_b.at[d], me, pair_peer)

    def copy_p(d):
        return remote(
            part.at[d, pl.ds(other_col * 2, 2)],
            pair_in.at[d],
            send_p.at[d],
            recv_p.at[d],
            me,
            pair_peer,
        )

    def copy_q(d):
        return remote(part.at[d, far_blk], col_in.at[d], send_q.at[d], recv_q.at[d], me, row_peer)

    def copy_r(d):
        return remote(
            part.at[d, own_blk], back.at[d], send_r.at[d], recv_r.at[d], partner(d), tp
        )

    @pl.loop(1, n)
    def _(d):
        copy_a(d).start()

        @pl.when(d < near)
        def _():
            copy_n(d).start()

    copy_k(near).start()

    @pl.loop(1, near)
    def _(d):
        copy_k(d).start()

    for fill in fills:
        fill.wait()

    def merge(index, other):
        rows = part.at[index]
        step = min(512, width)

        @pl.loop(0, width // step)
        def _(c):
            cols = pl.ds(pl.multiple_of(c * step, step), step)
            rows[:, cols] = (
                rows[:, cols].astype(jnp.float32) + other[:, cols].astype(jnp.float32)
            ).astype(part.dtype)

    def one_block(rows, put):
        gate = jnp.dot(rows, gate_ref[...], preferred_element_type=jnp.float32)
        up = jnp.dot(rows, up_ref[...], preferred_element_type=jnp.float32)
        hidden_ref[...] = (gate / (1.0 + jnp.exp(-gate)) * up).astype(hidden_ref.dtype)
        step = min(512, width)

        @pl.loop(0, width // step)
        def _(c):
            cols = pl.ds(pl.multiple_of(c * step, step), step)
            put(
                cols,
                jnp.dot(
                    hidden_ref[...], down_ref[:, cols], preferred_element_type=jnp.float32
                ).astype(part.dtype),
            )

    def compute(j):
        if slot_count % 16 == 0:

            def put(cols, val):
                part[j, :, :, cols] = val.reshape(4, slot_count, val.shape[1])

            one_block(slots[j].reshape(4 * slot_count, width), put)
        else:

            @pl.loop(0, 4)
            def _(b):
                def put(cols, val):
                    part[j, b, :, cols] = val

                one_block(slots[j, b], put)

    def inside(j, low):
        return jnp.logical_and(j >= low, j < n)

    @pl.loop(0, n + 5)
    def _(i):
        @pl.when(inside(i, 1))
        def _():
            copy_a(i).wait_recv()
            copy_c(i).start()

        @pl.when(inside(i, near))
        def _():
            copy_y(i).start()

        @pl.when(i == near)
        def _():
            copy_k(near).wait_recv()

            @pl.loop(near + 1, n)
            def _(d):
                copy_f(d).start()

        @pl.when(inside(i - 1, 1))
        def _():
            copy_y(i - 1).wait_recv()
            copy_b(i - 1).start()

        @pl.when(inside(i - 5, 0))
        def _():
            copy_q(i - 5).wait_recv()
            merge((i - 5, own_blk), col_in.at[i - 5])

        @pl.when(inside(i - 3, 0))
        def _():
            copy_p(i - 3).wait_recv()
            for y in range(2):
                merge((i - 3, col * 2 + y), pair_in.at[i - 3, y])

        @pl.when(inside(i - 2, 1))
        def _():
            copy_c(i - 2).wait_recv()
            copy_b(i - 2).wait_recv()

        @pl.when(inside(i - 2, 0))
        def _():
            compute(i - 2)

        @pl.when(inside(i - 5, 1))
        def _():
            copy_r(i - 5).start()

        @pl.when(inside(i - 3, 0))
        def _():
            copy_q(i - 3).start()

        @pl.when(inside(i - 2, 0))
        def _():
            copy_p(i - 2).start()

    def collect(d, rows):
        mix = mix_ref[d]
        high = mix.astype(jnp.bfloat16)
        low = (mix - high.astype(jnp.float32)).astype(jnp.bfloat16)
        both = jnp.dot(high, rows, preferred_element_type=jnp.float32) + jnp.dot(
            low, rows, preferred_element_type=jnp.float32
        )
        return both

    acc[...] = collect(0, part[0, own_blk])

    @pl.loop(1, n)
    def _(d):
        copy_r(d).wait_recv()
        acc[...] += collect(d, back[d])

    @pl.loop(1, near)
    def _(d):
        copy_k(d).wait()

    copy_k(near).wait_send()

    @pl.loop(near + 1, n)
    def _(d):
        copy_f(d).wait()

    keep.wait()
    res_ref[...] = acc[...].astype(res_ref.dtype)

    @pl.loop(1, n)
    def _(d):
        copy_a(d).wait_send()
        copy_y(d).wait_send()
        copy_c(d).wait_send()
        copy_b(d).wait_send()
        copy_r(d).wait_send()

    @pl.loop(0, n)
    def _(d):
        copy_p(d).wait_send()
        copy_q(d).wait_send()


def run_experts(outgoing, nearby, mine, kv, gate_w, up_w, down_w, mix):
    n, capacity, width = outgoing.shape
    hidden_units = gate_w.shape[1]
    tokens = mix.shape[1]
    rows = 4 * capacity if capacity % 16 == 0 else capacity
    dtype = outgoing.dtype
    vmem = pl.BlockSpec(memory_space=pltpu.VMEM)
    flops = 2 * n * 4 * capacity * width * hidden_units * 3
    return pl.pallas_call(
        functools.partial(expert_kernel, n),
        out_shape=(
            jax.ShapeDtypeStruct((tokens, width), dtype),
            jax.ShapeDtypeStruct((n,) + kv.shape, kv.dtype),
        ),
        in_specs=[vmem] * 8,
        out_specs=(vmem, pl.BlockSpec(memory_space=pl.ANY)),
        scratch_shapes=[
            pltpu.VMEM((n, 4, capacity, width), dtype),
            pltpu.VMEM((n, 4, capacity, width), dtype),
            pltpu.VMEM((n, 2, capacity, width), dtype),
            pltpu.VMEM((n, capacity, width), dtype),
            pltpu.VMEM((n, capacity, width), dtype),
            pltpu.VMEM((rows, hidden_units), dtype),
            pltpu.VMEM((tokens, width), jnp.float32),
        ]
        + [pltpu.SemaphoreType.DMA((n,))] * 16
        + [pltpu.SemaphoreType.DMA((5,))],
        compiler_params=pltpu.CompilerParams(
            collective_id=0, has_side_effects=True, vmem_limit_bytes=60 * 1024 * 1024
        ),
        cost_estimate=pl.CostEstimate(
            flops=40 * flops, bytes_accessed=16 * 1024 * 1024, transcendentals=0
        ),
    )(outgoing, nearby, mine, kv, gate_w, up_w, down_w, mix)


def expert_part(kv, moe_rows, moe_gain, routes, route_weights, w_gate, w_up, w_down):
    experts = lax.axis_size("ep")
    tp_count = lax.axis_size("tp")
    me = lax.axis_index("ep")
    tp_id = lax.axis_index("tp")
    dev_rows = moe_rows.shape[0] // tp_count
    top_count = routes.shape[1]
    capacity = max(2, 2 * dev_rows * top_count // experts)
    width = moe_rows.shape[1]
    normed = (
        rms_scaled(moe_rows.astype(jnp.float32), moe_gain)
        .astype(jnp.bfloat16)
        .reshape(tp_count, dev_rows, width)
    )
    relative = jnp.bitwise_xor(routes, me).reshape(tp_count, dev_rows, top_count)
    hits = relative[..., None] == lax.iota(jnp.int32, experts)
    named = jnp.any(hits, axis=2)
    before = (
        lax.iota(jnp.int32, dev_rows)[:, None] > lax.iota(jnp.int32, dev_rows)[None, :]
    ).astype(jnp.bfloat16)
    places = jnp.einsum(
        "ij,bjd->bid", before, named.astype(jnp.bfloat16), preferred_element_type=jnp.float32
    ).astype(jnp.int32)
    places = jnp.where(named, places, -1)
    slot_iota = lax.iota(jnp.int32, capacity)
    take_mine = (places[:, None, :, 0] == slot_iota[None, :, None]).astype(jnp.bfloat16)
    mine = jnp.einsum(
        "bst,btm->bsm", take_mine, normed, preferred_element_type=jnp.float32
    ).astype(jnp.bfloat16)
    own = lambda arr: lax.dynamic_index_in_dim(arr, tp_id, 0, keepdims=False)
    other_id = (1 - tp_id // 2) * 2 + tp_id % 2
    own_places = own(places)

    def fill(block, first, last):
        block_places = lax.dynamic_index_in_dim(places, block, 0, keepdims=False)[:, first:last]
        block_rows = lax.dynamic_index_in_dim(normed, block, 0, keepdims=False)
        take = (block_places.T[:, None, :] == slot_iota[None, :, None]).astype(jnp.bfloat16)
        return (
            jnp.dot(
                take.reshape(-1, dev_rows), block_rows, preferred_element_type=jnp.float32
            )
            .astype(jnp.bfloat16)
            .reshape(last - first, capacity, width)
        )

    outgoing = fill(tp_id, 0, experts)
    nearby = fill(other_id, 0, experts // 2)
    own_weights = own(route_weights.reshape(tp_count, dev_rows, top_count))
    weight_of = jnp.sum(jnp.where(own(hits), own_weights[..., None], 0.0), axis=1)
    mix = jnp.where(
        own_places.T[:, :, None] == slot_iota[None, None, :], weight_of.T[:, :, None], 0.0
    )
    return run_experts(outgoing, nearby, mine, kv, w_gate[0], w_up[0], w_down[0], mix)


def layer_kernel(
    n,
    rows_ref,
    gain_ref,
    places_ref,
    place_cols_ref,
    weight_cols_ref,
    q_ref,
    kv_ref,
    lam_ref,
    head_gain_ref,
    gate_hbm,
    up_hbm,
    down_hbm,
    w_out_hbm,
    mixer_ref,
    res_ref,
    gate_ref,
    up_ref,
    down_ref,
    w_out_ref,
    normed,
    packs,
    near_packs,
    kv_all,
    slots,
    part,
    pair_in,
    col_in,
    back,
    hidden_ref,
    acc,
    run_max,
    run_total,
    run_acc,
    attn,
    heads_all,
    send_k,
    recv_k,
    send_a,
    recv_a,
    send_y,
    recv_y,
    send_c,
    recv_c,
    send_b,
    recv_b,
    send_p,
    recv_p,
    send_q,
    recv_q,
    send_r,
    recv_r,
    send_h,
    recv_h,
    local_sem,
):
    me = lax.axis_index("ep")
    tp = lax.axis_index("tp")
    row = tp // 2
    col = tp % 2
    other_row = 1 - row
    other_col = 1 - col
    pair_peer = row * 2 + other_col
    row_peer = other_row * 2 + col
    own_blk = col * 2 + row
    far_blk = col * 2 + other_row
    slot_count = slots.shape[2]
    width = slots.shape[3]
    dev_rows = rows_ref.shape[1]
    step = min(512, width)
    near = n // 2
    bits = [1 << b for b in range(n.bit_length() - 1)]

    def partner(d):
        total = 0
        for bit in bits:
            total = total + (me // bit + d // bit) % 2 * bit
        return total

    def remote(src, dst, ssem, rsem, ep_id, tp_id):
        return pltpu.make_async_remote_copy(
            src_ref=src,
            dst_ref=dst,
            send_sem=ssem,
            recv_sem=rsem,
            device_id=(ep_id, tp_id),
            device_id_type=pl.DeviceIdType.MESH,
        )

    loads = [
        pltpu.make_async_copy(src, dst, local_sem.at[i])
        for i, (src, dst) in enumerate(
            (
                (gate_hbm, gate_ref),
                (up_hbm, up_ref),
                (down_hbm, down_ref),
                (kv_ref, kv_all.at[me]),
                (w_out_hbm, w_out_ref),
            )
        )
    ]
    for load in loads:
        load.start()

    barrier = pltpu.get_barrier_semaphore()

    @pl.loop(1, n)
    def _(d):
        pl.semaphore_signal(
            barrier, inc=1, device_id=(partner(d), tp), device_id_type=pl.DeviceIdType.MESH
        )

    @pl.loop(1, 4)
    def _(t):
        pl.semaphore_signal(
            barrier, inc=1, device_id=(me, (tp + t) % 4), device_id_type=pl.DeviceIdType.MESH
        )

    def norm_block(b):
        @pl.loop(0, dev_rows // 16)
        def _(r):
            piece = pl.ds(pl.multiple_of(r * 16, 16), 16)
            normed[b, piece, :] = rms_scaled(
                rows_ref[b, piece, :].astype(jnp.float32), gain_ref[...]
            ).astype(normed.dtype)

    slot_iota = lax.broadcasted_iota(jnp.int32, (slot_count, dev_rows), 0)

    def take(b, first, last):
        places = places_ref[b]
        return jnp.concatenate(
            [
                jnp.where(places[d : d + 1, :] == slot_iota, 1.0, 0.0)
                for d in range(first, last)
            ],
            axis=0,
        ).astype(jnp.bfloat16)

    def select(b, taken, put):
        @pl.loop(0, width // step)
        def _(c):
            cols = pl.ds(pl.multiple_of(c * step, step), step)
            put(
                cols,
                jnp.dot(
                    taken, normed[b, :, cols], preferred_element_type=jnp.float32
                ).astype(packs.dtype),
            )

    def copy_a(d):
        return remote(
            packs.at[d], slots.at[d, own_blk], send_a.at[d], recv_a.at[d], partner(d), tp
        )

    def copy_k(d):
        return remote(kv_ref, kv_all.at[me], send_k.at[d], recv_k.at[d], partner(d), tp)

    def copy_f(d):
        block = kv_all.at[partner(near)]
        return remote(block, block, send_k.at[d], recv_k.at[d], partner(d - near), tp)

    def copy_n(d):
        return remote(
            near_packs.at[d], slots.at[d, far_blk], send_y.at[d], recv_y.at[d], partner(d), tp
        )

    def copy_y(d):
        block = slots.at[d, own_blk]
        return remote(block, block, send_y.at[d], recv_y.at[d], me, row_peer)

    def copy_c(d):
        block = slots.at[d, own_blk]
        return remote(block, block, send_c.at[d], recv_c.at[d], me, pair_peer)

    def copy_b(d):
        block = slots.at[d, far_blk]
        return remote(block, block, send_b.at[d], recv_b.at[d], me, pair_peer)

    def copy_p(d):
        return remote(
            part.at[d, pl.ds(other_col * 2, 2)],
            pair_in.at[d],
            send_p.at[d],
            recv_p.at[d],
            me,
            pair_peer,
        )

    def copy_q(d):
        return remote(part.at[d, far_blk], col_in.at[d], send_q.at[d], recv_q.at[d], me, row_peer)

    def copy_r(d):
        return remote(
            part.at[d, own_blk], back.at[d], send_r.at[d], recv_r.at[d], partner(d), tp
        )

    positions = kv_ref.shape[0]
    piece_rows = positions // 4

    def copy_h(t):
        peer = (tp + t) % 4
        return remote(
            attn.at[pl.ds(pl.multiple_of(peer * piece_rows, piece_rows), piece_rows)],
            heads_all.at[tp],
            send_h.at[t],
            recv_h.at[t],
            me,
            peer,
        )

    norm_block(tp)

    def put_far(cols, val):
        packs[near:n, :, cols] = val.reshape(n - near, slot_count, val.shape[1])

    select(tp, take(tp, near, n), put_far)
    pl.semaphore_wait(barrier, n + 2)

    @pl.loop(near, n)
    def _(d):
        copy_a(d).start()

    loads[3].wait()
    low = me < near

    @pl.when(low)
    def _():
        copy_k(near).start()

    def put_near(cols, val):
        packs[0:near, :, cols] = val.reshape(near, slot_count, val.shape[1])

    select(tp, take(tp, 0, near), put_near)

    @pl.loop(1, near)
    def _(d):
        copy_a(d).start()

    norm_block(row_peer)

    def put_other(cols, val):
        near_packs[:, :, cols] = val.reshape(near, slot_count, val.shape[1])

    select(row_peer, take(row_peer, 0, near), put_other)

    @pl.loop(1, near)
    def _(d):
        copy_n(d).start()

        @pl.when(partner(d) > me)
        def _():
            copy_k(d).start()

    fills = [
        pltpu.make_async_copy(packs.at[0], slots.at[0, own_blk], local_sem.at[5]),
        pltpu.make_async_copy(near_packs.at[0], slots.at[0, far_blk], local_sem.at[6]),
    ]
    for fill in fills:
        fill.start()

    for peer_row in range(2):
        block = peer_row * 2 + other_col
        norm_block(block)

        def put_mine(cols, val, peer_row=peer_row):
            slots[0, other_col * 2 + peer_row, :, cols] = val

        select(block, take(block, 0, 1), put_mine)
    for fill in fills:
        fill.wait()
    for load in loads[:3]:
        load.wait()

    def merge(index, other):
        rows = part.at[index]

        @pl.loop(0, width // step)
        def _(c):
            cols = pl.ds(pl.multiple_of(c * step, step), step)
            rows[:, cols] = (
                rows[:, cols].astype(jnp.float32) + other[:, cols].astype(jnp.float32)
            ).astype(part.dtype)

    def compute(j):
        rows = slots[j].reshape(4 * slot_count, width)
        gate = jnp.dot(rows, gate_ref[...], preferred_element_type=jnp.float32)
        up = jnp.dot(rows, up_ref[...], preferred_element_type=jnp.float32)
        hidden_ref[...] = (gate / (1.0 + jnp.exp(-gate)) * up).astype(hidden_ref.dtype)

        @pl.loop(0, width // step)
        def _(c):
            cols = pl.ds(pl.multiple_of(c * step, step), step)
            val = jnp.dot(
                hidden_ref[...], down_ref[:, cols], preferred_element_type=jnp.float32
            ).astype(part.dtype)
            part[j, :, :, cols] = val.reshape(4, slot_count, step)

    def order(i):
        far_step = near + i - 1
        return jnp.where(i <= 0, 0, jnp.where(i <= near, far_step, i - near))

    def inside(j, low_bound):
        return jnp.logical_and(j >= low_bound, j < n)

    @pl.loop(0, n + 2)
    def _(i):
        d_in = order(i)
        d_mid = order(i - 1)
        d_out = order(i - 2)

        @pl.when(inside(i, 1))
        def _():
            copy_a(d_in).wait_recv()
            copy_c(d_in).start()

            @pl.when(d_in >= near)
            def _():
                copy_y(d_in).start()

        @pl.when(inside(i - 1, 1))
        def _():
            copy_y(d_mid).wait_recv()
            copy_b(d_mid).start()
            copy_c(d_mid).wait_recv()
            copy_b(d_mid).wait_recv()

        @pl.when(inside(i - 1, 0))
        def _():
            compute(d_mid)
            copy_p(d_mid).start()

        @pl.when(inside(i - 2, 0))
        def _():
            copy_q(d_out).wait_recv()
            merge((d_out, own_blk), col_in.at[d_out])

        @pl.when(inside(i - 2, 1))
        def _():
            copy_r(d_out).start()

        @pl.when(inside(i - 1, 0))
        def _():
            copy_p(d_mid).wait_recv()
            for y in range(2):
                merge((d_mid, col * 2 + y), pair_in.at[d_mid, y])
            copy_q(d_mid).start()

        @pl.when(jnp.logical_and(i == near + 1, jnp.logical_not(low)))
        def _():
            copy_k(near).wait_recv()

            @pl.loop(near + 1, n)
            def _(d):
                copy_f(d).start()

    @pl.loop(1, near)
    def _(d):
        @pl.when(partner(d) < me)
        def _():
            copy_k(d).wait_recv()

    @pl.when(jnp.logical_not(low))
    def _():
        @pl.loop(near + 1, n)
        def _(d):
            copy_f(d).wait_recv()

    head_dim2 = kv_ref.shape[1] // 2
    q_heads = q_ref.shape[1] // head_dim2
    inv_scale = (head_dim2 // 2) ** (-0.5)
    run_max[...] = jnp.full(run_max.shape, MASKED, jnp.float32)
    run_total[...] = jnp.zeros(run_total.shape, jnp.float32)
    run_acc[...] = jnp.zeros(run_acc.shape, jnp.float32)
    map_of = lax.broadcasted_iota(jnp.int32, (positions, head_dim2), 1) // (head_dim2 // 2)

    @pl.loop(0, me + 1)
    def _(kb):
        keys = kv_all[kb, :, :head_dim2]
        vals = kv_all[kb, :, head_dim2:]
        gap = (me - kb) * positions
        allowed = (
            lax.broadcasted_iota(jnp.int32, (positions, positions), 1)
            <= lax.broadcasted_iota(jnp.int32, (positions, positions), 0) + gap
        )
        for h in range(q_heads):
            for m in range(2):
                at = h * 2 + m
                query = q_ref[:, h * head_dim2 : (h + 1) * head_dim2]
                query = jnp.where(map_of == m, query, jnp.zeros_like(query))
                scores = (
                    lax.dot_general(
                        query, keys, (((1,), (1,)), ((), ())), preferred_element_type=jnp.float32
                    )
                    * inv_scale
                )
                scores = jnp.where(allowed, scores, MASKED)
                old_max = run_max[at]
                new_max = jnp.maximum(old_max, jnp.max(scores, axis=1, keepdims=True))
                shrink = jnp.exp(old_max - new_max)
                weights = jnp.exp(scores - new_max)
                run_max[at] = new_max
                run_total[at] = run_total[at] * shrink + jnp.sum(weights, axis=1, keepdims=True)
                run_acc[at] = run_acc[at] * shrink + jnp.dot(
                    weights.astype(jnp.bfloat16), vals, preferred_element_type=jnp.float32
                )

    for h in range(q_heads):
        head_out = (
            run_acc[2 * h] / run_total[2 * h]
            - lam_ref[h] * run_acc[2 * h + 1] / run_total[2 * h + 1]
        )
        attn[:, h * head_dim2 : (h + 1) * head_dim2] = rms_scaled(
            head_out, head_gain_ref[...]
        ).astype(attn.dtype)

    for t in range(1, 4):
        copy_h(t).start()
    heads_all[tp] = attn[pl.ds(pl.multiple_of(tp * piece_rows, piece_rows), piece_rows), :]

    def collect(d, rows):
        lanes = lax.broadcasted_iota(jnp.int32, place_cols_ref.shape, 1)
        place = jnp.sum(jnp.where(lanes == d, place_cols_ref[...], 0), axis=1, keepdims=True)
        weight = jnp.sum(jnp.where(lanes == d, weight_cols_ref[...], 0.0), axis=1, keepdims=True)
        slot = lax.broadcasted_iota(jnp.int32, (dev_rows, slot_count), 1)
        mix = jnp.where(slot == place, weight, 0.0)
        high = mix.astype(jnp.bfloat16)
        low_part = (mix - high.astype(jnp.float32)).astype(jnp.bfloat16)

        @pl.loop(0, width // step)
        def _(c):
            cols = pl.ds(pl.multiple_of(c * step, step), step)
            piece = rows[:, cols]
            acc[:, cols] += jnp.dot(high, piece, preferred_element_type=jnp.float32) + jnp.dot(
                low_part, piece, preferred_element_type=jnp.float32
            )

    acc[...] = jnp.zeros(acc.shape, jnp.float32)
    collect(0, part.at[0, own_blk])

    @pl.loop(1, near)
    def _(d):
        copy_r(d).wait_recv()
        collect(d, back.at[d])

    loads[4].wait()
    for t in range(1, 4):
        copy_h(t).wait_recv()
    mixed = heads_all.shape[2]

    @pl.loop(0, width // step)
    def _(c):
        cols = pl.ds(pl.multiple_of(c * step, step), step)
        total = jnp.zeros((piece_rows, step), jnp.float32)
        for t in range(4):
            total = total + jnp.dot(
                heads_all[t],
                w_out_ref[t * mixed : (t + 1) * mixed, cols],
                preferred_element_type=jnp.float32,
            )
        mixer_ref[:, cols] = total.astype(mixer_ref.dtype)

    @pl.loop(near, n)
    def _(d):
        copy_r(d).wait_recv()
        collect(d, back.at[d])

    res_ref[...] = acc[...].astype(res_ref.dtype)

    @pl.when(low)
    def _():
        copy_k(near).wait_send()

    @pl.loop(1, near)
    def _(d):
        copy_n(d).wait_send()

        @pl.when(partner(d) > me)
        def _():
            copy_k(d).wait_send()

    @pl.when(jnp.logical_not(low))
    def _():
        @pl.loop(near + 1, n)
        def _(d):
            copy_f(d).wait_send()

    @pl.loop(near, n)
    def _(d):
        copy_y(d).wait_send()

    @pl.loop(1, n)
    def _(d):
        copy_a(d).wait_send()
        copy_c(d).wait_send()
        copy_b(d).wait_send()
        copy_r(d).wait_send()

    @pl.loop(0, n)
    def _(d):
        copy_p(d).wait_send()
        copy_q(d).wait_send()

    for t in range(1, 4):
        copy_h(t).wait_send()


def run_layer(n, capacity, rows, gain, places, place_cols, weight_cols, q, kv, lam, head_gain, mats):
    tp_count, dev_rows, width = rows.shape
    gate_w, up_w, down_w, w_out = mats
    hidden_units = gate_w.shape[1]
    positions, mixed = q.shape
    head_dim2 = kv.shape[1] // 2
    maps = 2 * mixed // head_dim2
    dtype = rows.dtype
    near = n // 2
    vmem = pl.BlockSpec(memory_space=pltpu.VMEM)
    hbm = pl.BlockSpec(memory_space=pl.ANY)
    flops = 2 * n * 4 * capacity * width * hidden_units * 3
    return pl.pallas_call(
        functools.partial(layer_kernel, n),
        out_shape=(
            jax.ShapeDtypeStruct((positions // tp_count, width), dtype),
            jax.ShapeDtypeStruct((dev_rows, width), dtype),
        ),
        in_specs=[vmem] * 7 + [pl.BlockSpec(memory_space=pltpu.SMEM), vmem] + [hbm] * 4,
        out_specs=(vmem, vmem),
        scratch_shapes=[
            pltpu.VMEM(gate_w.shape, dtype),
            pltpu.VMEM(up_w.shape, dtype),
            pltpu.VMEM(down_w.shape, dtype),
            pltpu.VMEM(w_out.shape, dtype),
            pltpu.VMEM((tp_count, dev_rows, width), dtype),
            pltpu.VMEM((n, capacity, width), dtype),
            pltpu.VMEM((near, capacity, width), dtype),
            pltpu.VMEM((n,) + kv.shape, dtype),
            pltpu.VMEM((n, 4, capacity, width), dtype),
            pltpu.VMEM((n, 4, capacity, width), dtype),
            pltpu.VMEM((n, 2, capacity, width), dtype),
            pltpu.VMEM((n, capacity, width), dtype),
            pltpu.VMEM((n, capacity, width), dtype),
            pltpu.VMEM((4 * capacity, hidden_units), dtype),
            pltpu.VMEM((dev_rows, width), jnp.float32),
            pltpu.VMEM((maps, positions, 1), jnp.float32),
            pltpu.VMEM((maps, positions, 1), jnp.float32),
            pltpu.VMEM((maps, positions, head_dim2), jnp.float32),
            pltpu.VMEM((positions, mixed), dtype),
            pltpu.VMEM((tp_count, positions // tp_count, mixed), dtype),
        ]
        + [pltpu.SemaphoreType.DMA((n,))] * 16
        + [pltpu.SemaphoreType.DMA((4,))] * 2
        + [pltpu.SemaphoreType.DMA((7,))],
        compiler_params=pltpu.CompilerParams(
            collective_id=1, has_side_effects=True, vmem_limit_bytes=60 * 1024 * 1024
        ),
        cost_estimate=pl.CostEstimate(
            flops=40 * flops, bytes_accessed=16 * 1024 * 1024, transcendentals=0
        ),
    )(rows, gain, places, place_cols, weight_cols, q, kv, lam, head_gain, *mats)


def one_kernel(
    queries,
    keys,
    values,
    attn_lambda,
    head_gain,
    w_out,
    moe_rows,
    moe_gain,
    routes,
    route_weights,
    w_gate,
    w_up,
    w_down,
):
    experts = lax.axis_size("ep")
    tp_count = lax.axis_size("tp")
    me = lax.axis_index("ep")
    tp_id = lax.axis_index("tp")
    positions = queries.shape[0]
    width = moe_rows.shape[1]
    dev_rows = moe_rows.shape[0] // tp_count
    top_count = routes.shape[1]
    capacity = 2 * dev_rows * top_count // experts
    relative = jnp.bitwise_xor(routes, me).reshape(tp_count, dev_rows, top_count)
    hits = relative[..., None] == lax.iota(jnp.int32, experts)
    named = jnp.any(hits, axis=2)
    before = (
        lax.iota(jnp.int32, dev_rows)[:, None] > lax.iota(jnp.int32, dev_rows)[None, :]
    ).astype(jnp.bfloat16)
    places = jnp.einsum(
        "ij,bjd->bid", before, named.astype(jnp.bfloat16), preferred_element_type=jnp.float32
    ).astype(jnp.int32)
    places = jnp.where(named, places, -1)
    own = lambda arr: lax.dynamic_index_in_dim(arr, tp_id, 0, keepdims=False)
    own_weights = own(route_weights.reshape(tp_count, dev_rows, top_count))
    weight_cols = jnp.sum(jnp.where(own(hits), own_weights[..., None], 0.0), axis=1)
    kv = jnp.concatenate([keys, values], axis=2).reshape(positions, -1)
    return run_layer(
        experts,
        capacity,
        moe_rows.reshape(tp_count, dev_rows, width),
        moe_gain.reshape(1, width),
        jnp.transpose(places, (0, 2, 1)),
        own(places),
        weight_cols,
        queries.reshape(positions, -1),
        kv,
        attn_lambda,
        head_gain.reshape(1, -1),
        (w_gate[0], w_up[0], w_down[0], w_out),
    )


def local(
    queries,
    keys,
    values,
    attn_lambda,
    head_gain,
    w_out,
    moe_rows,
    moe_gain,
    routes,
    route_weights,
    w_gate,
    w_up,
    w_down,
):
    positions = queries.shape[0]
    q_heads = queries.shape[1]
    kv_heads = keys.shape[1]
    head_dim = queries.shape[2] // 2
    value_dim = values.shape[2]
    per_key = q_heads // kv_heads
    first_pos = lax.axis_index("ep") * positions
    query_pos = first_pos + lax.iota(jnp.int32, positions)
    last_pos = first_pos + positions - 1
    query_view = queries.reshape(positions, kv_heads, per_key, 2, head_dim)
    inv_scale = head_dim ** (-0.5)
    start_max = jnp.full((positions, kv_heads, per_key, 2), MASKED, jnp.float32)
    start_total = jnp.zeros((positions, kv_heads, per_key, 2), jnp.float32)
    start_acc = jnp.zeros((positions, kv_heads, per_key, 2, value_dim), jnp.float32)
    carry = (start_max, start_total, start_acc)
    both = jnp.concatenate([keys, values], axis=2)
    moe_out, gathered = expert_part(
        both.reshape(positions, -1),
        moe_rows,
        moe_gain,
        routes,
        route_weights,
        w_gate,
        w_up,
        w_down,
    )
    gathered = gathered.reshape(-1, kv_heads, both.shape[2])
    key_piece = gathered[:, :, : keys.shape[2]]
    value_piece = gathered[:, :, keys.shape[2] :]
    shard_count = key_piece.shape[0] // positions
    together = 1
    for candidate in (2, 3, 4):
        if shard_count % candidate == 0:
            together = candidate
    block_len = together * positions
    blocks = shard_count // together
    key_blocks = key_piece.reshape(blocks, block_len, kv_heads, 2, head_dim)
    value_blocks = value_piece.reshape(blocks, block_len, kv_heads, value_dim)
    block_starts = block_len * lax.iota(jnp.int32, blocks)

    def visit(running, inputs):
        key_blk, value_blk, block_start = inputs

        def update(current):
            run_max, run_total, run_acc = current
            key_pos = block_start + lax.iota(jnp.int32, block_len)
            scores = (
                jnp.einsum(
                    "qkgmd,pkmd->qkgmp", query_view, key_blk, preferred_element_type=jnp.float32
                )
                * inv_scale
            )
            allowed = key_pos[None, :] <= query_pos[:, None]
            scores = jnp.where(allowed[:, None, None, None, :], scores, MASKED)
            new_max = jnp.maximum(run_max, jnp.max(scores, axis=-1))
            shrink = jnp.exp(run_max - new_max)
            weights = jnp.exp(scores - new_max[..., None])
            run_total = run_total * shrink + jnp.sum(weights, axis=-1)
            run_acc = run_acc * shrink[..., None] + jnp.einsum(
                "qkgmp,pkv->qkgmv",
                weights.astype(jnp.bfloat16),
                value_blk,
                preferred_element_type=jnp.float32,
            )
            return (new_max, run_total, run_acc)

        def keep(current):
            return current

        return (lax.cond(block_start <= last_pos, update, keep, running), None)

    carry, unused = lax.scan(visit, carry, (key_blocks, value_blocks, block_starts))
    run_max, run_total, run_acc = carry
    ratios = run_acc / run_total[..., None]
    lambda_view = attn_lambda.reshape(1, kv_heads, per_key, 1)
    head_out = ratios[:, :, :, 0] - lambda_view * ratios[:, :, :, 1]
    attn_rows = (
        rms_scaled(head_out, head_gain).astype(jnp.bfloat16).reshape(positions, q_heads * value_dim)
    )
    tp_count = lax.axis_size("tp")
    tp_id = lax.axis_index("tp")
    exchanged = lax.all_to_all(
        attn_rows.reshape(positions, q_heads, value_dim),
        "tp",
        split_axis=0,
        concat_axis=1,
        tiled=True,
    )
    mixer_out = jnp.dot(
        exchanged.reshape(positions // tp_count, tp_count * q_heads * value_dim),
        w_out,
        preferred_element_type=jnp.float32,
    ).astype(jnp.bfloat16)
    return (mixer_out, moe_out)


def solution(mesh):
    experts, tp_count = mesh.shape["ep"], mesh.shape["tp"]

    def body(*args):
        keys, moe_rows, routes = args[1], args[6], args[8]
        capacity = 2 * (moe_rows.shape[0] // tp_count) * routes.shape[1] // experts
        whole_tiles = capacity % 16 == 0 and keys.shape[1] == 1
        return (one_kernel if whole_tiles else local)(*args)

    return jax.shard_map(
        body,
        mesh=mesh,
        in_specs=(
            P("ep", "tp", None),
            P("ep", "tp", None),
            P("ep", "tp", None),
            P("tp"),
            P(),
            P(),
            P("ep", None),
            P(),
            P("ep", None),
            P("ep", None),
            P("ep", None, "tp"),
            P("ep", None, "tp"),
            P("ep", "tp", None),
        ),
        out_specs=(P(("ep", "tp"), None), P(("ep", "tp"), None)),
        check_vma=False,
    )
```

```python
import functools

import jax
import jax.numpy as jnp
from jax import lax
from jax.experimental import pallas as pl
from jax.experimental.pallas import tpu as pltpu
from jax.sharding import PartitionSpec as P

EPSILON = 1e-06
MASKED = -1e30


def rms_scaled(values_f, gain):
    mean_sq = jnp.mean(values_f * values_f, axis=-1, keepdims=True)
    return values_f * lax.rsqrt(mean_sq + EPSILON) * gain


def expert_kernel(
    n,
    out_ref,
    near_ref,
    mine_ref,
    kv_ref,
    gate_ref,
    up_ref,
    down_ref,
    mix_ref,
    res_ref,
    kv_out,
    slots,
    part,
    pair_in,
    col_in,
    back,
    hidden_ref,
    acc,
    send_k,
    recv_k,
    send_a,
    recv_a,
    send_y,
    recv_y,
    send_c,
    recv_c,
    send_b,
    recv_b,
    send_p,
    recv_p,
    send_q,
    recv_q,
    send_r,
    recv_r,
    local_sem,
):
    me = lax.axis_index("ep")
    tp = lax.axis_index("tp")
    row = tp // 2
    col = tp % 2
    other_row = 1 - row
    other_col = 1 - col
    pair_peer = row * 2 + other_col
    row_peer = other_row * 2 + col
    own_blk = col * 2 + row
    far_blk = col * 2 + other_row
    slot_count = slots.shape[2]
    width = slots.shape[3]

    near = near_ref.shape[0]
    bits = [1 << b for b in range(n.bit_length() - 1)]

    def partner(d):
        total = 0
        for bit in bits:
            total = total + (me // bit + d // bit) % 2 * bit
        return total

    def remote(src, dst, ssem, rsem, ep_id, tp_id):
        return pltpu.make_async_remote_copy(
            src_ref=src,
            dst_ref=dst,
            send_sem=ssem,
            recv_sem=rsem,
            device_id=(ep_id, tp_id),
            device_id_type=pl.DeviceIdType.MESH,
        )

    barrier = pltpu.get_barrier_semaphore()

    @pl.loop(1, n)
    def _(d):
        pl.semaphore_signal(
            barrier, inc=1, device_id=(partner(d), tp), device_id_type=pl.DeviceIdType.MESH
        )

    for peer in (pair_peer, row_peer):
        pl.semaphore_signal(
            barrier, inc=1, device_id=(me, peer), device_id_type=pl.DeviceIdType.MESH
        )
    keep = pltpu.make_async_copy(kv_ref, kv_out.at[me], local_sem.at[4])
    keep.start()
    fills = [
        pltpu.make_async_copy(
            mine_ref.at[b], slots.at[0, (b % 2) * 2 + b // 2], local_sem.at[b]
        )
        for b in range(4)
    ]
    for fill in fills:
        fill.start()
    pl.semaphore_wait(barrier, n + 1)

    def copy_a(d):
        return remote(
            out_ref.at[d], slots.at[d, own_blk], send_a.at[d], recv_a.at[d], partner(d), tp
        )

    def copy_k(d):
        return remote(kv_ref, kv_out.at[me], send_k.at[d], recv_k.at[d], partner(d), tp)

    def copy_f(d):
        block = kv_out.at[partner(near)]
        return remote(block, block, send_k.at[d], recv_k.at[d], partner(d - near), tp)

    def copy_n(d):
        return remote(
            near_ref.at[d], slots.at[d, far_blk], send_y.at[d], recv_y.at[d], partner(d), tp
        )

    def copy_y(d):
        block = slots.at[d, own_blk]
        return remote(block, block, send_y.at[d], recv_y.at[d], me, row_peer)

    def copy_c(d):
        block = slots.at[d, own_blk]
        return remote(block, block, send_c.at[d], recv_c.at[d], me, pair_peer)

    def copy_b(d):
        block = slots.at[d, far_blk]
        return remote(block, block, send_b.at[d], recv_b.at[d], me, pair_peer)

    def copy_p(d):
        return remote(
            part.at[d, pl.ds(other_col * 2, 2)],
            pair_in.at[d],
            send_p.at[d],
            recv_p.at[d],
            me,
            pair_peer,
        )

    def copy_q(d):
        return remote(part.at[d, far_blk], col_in.at[d], send_q.at[d], recv_q.at[d], me, row_peer)

    def copy_r(d):
        return remote(
            part.at[d, own_blk], back.at[d], send_r.at[d], recv_r.at[d], partner(d), tp
        )

    @pl.loop(1, n)
    def _(d):
        copy_a(d).start()

        @pl.when(d < near)
        def _():
            copy_n(d).start()

    copy_k(near).start()

    @pl.loop(1, near)
    def _(d):
        copy_k(d).start()

    for fill in fills:
        fill.wait()

    def merge(index, other):
        rows = part.at[index]
        step = min(512, width)

        @pl.loop(0, width // step)
        def _(c):
            cols = pl.ds(pl.multiple_of(c * step, step), step)
            rows[:, cols] = (
                rows[:, cols].astype(jnp.float32) + other[:, cols].astype(jnp.float32)
            ).astype(part.dtype)

    def one_block(rows, put):
        gate = jnp.dot(rows, gate_ref[...], preferred_element_type=jnp.float32)
        up = jnp.dot(rows, up_ref[...], preferred_element_type=jnp.float32)
        hidden_ref[...] = (gate / (1.0 + jnp.exp(-gate)) * up).astype(hidden_ref.dtype)
        step = min(512, width)

        @pl.loop(0, width // step)
        def _(c):
            cols = pl.ds(pl.multiple_of(c * step, step), step)
            put(
                cols,
                jnp.dot(
                    hidden_ref[...], down_ref[:, cols], preferred_element_type=jnp.float32
                ).astype(part.dtype),
            )

    def compute(j):
        if slot_count % 16 == 0:

            def put(cols, val):
                part[j, :, :, cols] = val.reshape(4, slot_count, val.shape[1])

            one_block(slots[j].reshape(4 * slot_count, width), put)
        else:

            @pl.loop(0, 4)
            def _(b):
                def put(cols, val):
                    part[j, b, :, cols] = val

                one_block(slots[j, b], put)

    def inside(j, low):
        return jnp.logical_and(j >= low, j < n)

    @pl.loop(0, n + 5)
    def _(i):
        @pl.when(inside(i, 1))
        def _():
            copy_a(i).wait_recv()
            copy_c(i).start()

        @pl.when(inside(i, near))
        def _():
            copy_y(i).start()

        @pl.when(i == near)
        def _():
            copy_k(near).wait_recv()

            @pl.loop(near + 1, n)
            def _(d):
                copy_f(d).start()

        @pl.when(inside(i - 1, 1))
        def _():
            copy_y(i - 1).wait_recv()
            copy_b(i - 1).start()

        @pl.when(inside(i - 5, 0))
        def _():
            copy_q(i - 5).wait_recv()
            merge((i - 5, own_blk), col_in.at[i - 5])

        @pl.when(inside(i - 3, 0))
        def _():
            copy_p(i - 3).wait_recv()
            for y in range(2):
                merge((i - 3, col * 2 + y), pair_in.at[i - 3, y])

        @pl.when(inside(i - 2, 1))
        def _():
            copy_c(i - 2).wait_recv()
            copy_b(i - 2).wait_recv()

        @pl.when(inside(i - 2, 0))
        def _():
            compute(i - 2)

        @pl.when(inside(i - 5, 1))
        def _():
            copy_r(i - 5).start()

        @pl.when(inside(i - 3, 0))
        def _():
            copy_q(i - 3).start()

        @pl.when(inside(i - 2, 0))
        def _():
            copy_p(i - 2).start()

    def collect(d, rows):
        mix = mix_ref[d]
        high = mix.astype(jnp.bfloat16)
        low = (mix - high.astype(jnp.float32)).astype(jnp.bfloat16)
        both = jnp.dot(high, rows, preferred_element_type=jnp.float32) + jnp.dot(
            low, rows, preferred_element_type=jnp.float32
        )
        return both

    acc[...] = collect(0, part[0, own_blk])

    @pl.loop(1, n)
    def _(d):
        copy_r(d).wait_recv()
        acc[...] += collect(d, back[d])

    @pl.loop(1, near)
    def _(d):
        copy_k(d).wait()

    copy_k(near).wait_send()

    @pl.loop(near + 1, n)
    def _(d):
        copy_f(d).wait()

    keep.wait()
    res_ref[...] = acc[...].astype(res_ref.dtype)

    @pl.loop(1, n)
    def _(d):
        copy_a(d).wait_send()
        copy_y(d).wait_send()
        copy_c(d).wait_send()
        copy_b(d).wait_send()
        copy_r(d).wait_send()

    @pl.loop(0, n)
    def _(d):
        copy_p(d).wait_send()
        copy_q(d).wait_send()


def run_experts(outgoing, nearby, mine, kv, gate_w, up_w, down_w, mix):
    n, capacity, width = outgoing.shape
    hidden_units = gate_w.shape[1]
    tokens = mix.shape[1]
    rows = 4 * capacity if capacity % 16 == 0 else capacity
    dtype = outgoing.dtype
    vmem = pl.BlockSpec(memory_space=pltpu.VMEM)
    flops = 2 * n * 4 * capacity * width * hidden_units * 3
    return pl.pallas_call(
        functools.partial(expert_kernel, n),
        out_shape=(
            jax.ShapeDtypeStruct((tokens, width), dtype),
            jax.ShapeDtypeStruct((n,) + kv.shape, kv.dtype),
        ),
        in_specs=[vmem] * 8,
        out_specs=(vmem, pl.BlockSpec(memory_space=pl.ANY)),
        scratch_shapes=[
            pltpu.VMEM((n, 4, capacity, width), dtype),
            pltpu.VMEM((n, 4, capacity, width), dtype),
            pltpu.VMEM((n, 2, capacity, width), dtype),
            pltpu.VMEM((n, capacity, width), dtype),
            pltpu.VMEM((n, capacity, width), dtype),
            pltpu.VMEM((rows, hidden_units), dtype),
            pltpu.VMEM((tokens, width), jnp.float32),
        ]
        + [pltpu.SemaphoreType.DMA((n,))] * 16
        + [pltpu.SemaphoreType.DMA((5,))],
        compiler_params=pltpu.CompilerParams(
            collective_id=0, has_side_effects=True, vmem_limit_bytes=60 * 1024 * 1024
        ),
        cost_estimate=pl.CostEstimate(
            flops=40 * flops, bytes_accessed=16 * 1024 * 1024, transcendentals=0
        ),
    )(outgoing, nearby, mine, kv, gate_w, up_w, down_w, mix)


def expert_part(kv, moe_rows, moe_gain, routes, route_weights, w_gate, w_up, w_down):
    experts = lax.axis_size("ep")
    tp_count = lax.axis_size("tp")
    me = lax.axis_index("ep")
    tp_id = lax.axis_index("tp")
    dev_rows = moe_rows.shape[0] // tp_count
    top_count = routes.shape[1]
    capacity = max(2, 2 * dev_rows * top_count // experts)
    width = moe_rows.shape[1]
    normed = (
        rms_scaled(moe_rows.astype(jnp.float32), moe_gain)
        .astype(jnp.bfloat16)
        .reshape(tp_count, dev_rows, width)
    )
    relative = jnp.bitwise_xor(routes, me).reshape(tp_count, dev_rows, top_count)
    hits = relative[..., None] == lax.iota(jnp.int32, experts)
    named = jnp.any(hits, axis=2)
    before = (
        lax.iota(jnp.int32, dev_rows)[:, None] > lax.iota(jnp.int32, dev_rows)[None, :]
    ).astype(jnp.bfloat16)
    places = jnp.einsum(
        "ij,bjd->bid", before, named.astype(jnp.bfloat16), preferred_element_type=jnp.float32
    ).astype(jnp.int32)
    places = jnp.where(named, places, -1)
    slot_iota = lax.iota(jnp.int32, capacity)
    take_mine = (places[:, None, :, 0] == slot_iota[None, :, None]).astype(jnp.bfloat16)
    mine = jnp.einsum(
        "bst,btm->bsm", take_mine, normed, preferred_element_type=jnp.float32
    ).astype(jnp.bfloat16)
    own = lambda arr: lax.dynamic_index_in_dim(arr, tp_id, 0, keepdims=False)
    other_id = (1 - tp_id // 2) * 2 + tp_id % 2
    own_places = own(places)

    def fill(block, first, last):
        block_places = lax.dynamic_index_in_dim(places, block, 0, keepdims=False)[:, first:last]
        block_rows = lax.dynamic_index_in_dim(normed, block, 0, keepdims=False)
        take = (block_places.T[:, None, :] == slot_iota[None, :, None]).astype(jnp.bfloat16)
        return (
            jnp.dot(
                take.reshape(-1, dev_rows), block_rows, preferred_element_type=jnp.float32
            )
            .astype(jnp.bfloat16)
            .reshape(last - first, capacity, width)
        )

    outgoing = fill(tp_id, 0, experts)
    nearby = fill(other_id, 0, experts // 2)
    own_weights = own(route_weights.reshape(tp_count, dev_rows, top_count))
    weight_of = jnp.sum(jnp.where(own(hits), own_weights[..., None], 0.0), axis=1)
    mix = jnp.where(
        own_places.T[:, :, None] == slot_iota[None, None, :], weight_of.T[:, :, None], 0.0
    )
    return run_experts(outgoing, nearby, mine, kv, w_gate[0], w_up[0], w_down[0], mix)


def layer_kernel(
    n,
    rows_ref,
    gain_ref,
    routes_ref,
    weights_ref,
    q_ref,
    key_ref,
    value_ref,
    lam_ref,
    head_gain_ref,
    gate_hbm,
    up_hbm,
    down_hbm,
    w_out_hbm,
    mixer_ref,
    res_ref,
    gate_ref,
    up_ref,
    down_ref,
    w_out_ref,
    normed,
    packs,
    near_packs,
    far_rows,
    places_ref,
    far_places,
    scaled_ref,
    cols_ref,
    query_ref,
    kv_ref,
    kv_all,
    slots,
    part,
    pair_in,
    back,
    hidden_ref,
    hidden_in,
    down_peer,
    acc,
    run_max,
    run_total,
    run_acc,
    head_rows,
    attn,
    heads_all,
    send_k,
    recv_k,
    send_a,
    recv_a,
    send_y,
    recv_y,
    send_c,
    recv_c,
    send_b,
    recv_b,
    send_p,
    recv_p,
    send_q,
    recv_q,
    send_r,
    recv_r,
    send_h,
    recv_h,
    send_x,
    recv_x,
    local_sem,
):
    me = lax.axis_index("ep")
    tp = lax.axis_index("tp")
    row = tp // 2
    col = tp % 2
    other_row = 1 - row
    other_col = 1 - col
    pair_peer = row * 2 + other_col
    row_peer = other_row * 2 + col
    own_blk = col * 2 + row
    far_blk = col * 2 + other_row
    slot_count = slots.shape[2]
    width = slots.shape[3]
    dev_rows = rows_ref.shape[1]
    step = min(512, width)
    near = n // 2
    bits = [1 << b for b in range(n.bit_length() - 1)]

    def partner(d):
        total = 0
        for bit in bits:
            total = total + (me // bit + d // bit) % 2 * bit
        return total

    def remote(src, dst, ssem, rsem, ep_id, tp_id):
        return pltpu.make_async_remote_copy(
            src_ref=src,
            dst_ref=dst,
            send_sem=ssem,
            recv_sem=rsem,
            device_id=(ep_id, tp_id),
            device_id_type=pl.DeviceIdType.MESH,
        )

    loads = [
        pltpu.make_async_copy(src, dst, local_sem.at[i])
        for i, (src, dst) in enumerate(
            (
                (gate_hbm, gate_ref),
                (up_hbm, up_ref),
                (down_hbm, down_ref),
                (w_out_hbm, w_out_ref),
            )
        )
    ]
    for load in loads:
        load.start()

    barrier = pltpu.get_barrier_semaphore()

    @pl.loop(1, n)
    def _(d):
        pl.semaphore_signal(
            barrier, inc=1, device_id=(partner(d), tp), device_id_type=pl.DeviceIdType.MESH
        )

    @pl.loop(1, 4)
    def _(t):
        pl.semaphore_signal(
            barrier, inc=1, device_id=(me, (tp + t) % 4), device_id_type=pl.DeviceIdType.MESH
        )

    def norm_block(b):
        @pl.loop(0, dev_rows // 16)
        def _(r):
            piece = pl.ds(pl.multiple_of(r * 16, 16), 16)
            normed[b, piece, :] = rms_scaled(
                rows_ref[b, piece, :].astype(jnp.float32), gain_ref[...]
            ).astype(normed.dtype)

    slot_iota = lax.broadcasted_iota(jnp.int32, (slot_count, dev_rows), 0)

    def take(places, first, last):
        return jnp.concatenate(
            [
                jnp.where(places[d : d + 1, :] == slot_iota, 1.0, 0.0)
                for d in range(first, last)
            ],
            axis=0,
        ).astype(jnp.bfloat16)

    def select(source, taken, put, first=0, last=width // step):
        for c in range(first, last):
            cols = pl.ds(c * step, step)
            put(
                cols,
                jnp.dot(
                    taken, source[:, cols], preferred_element_type=jnp.float32
                ).astype(packs.dtype),
            )

    def copy_x(half):
        cols = pl.ds(half * (width // 2), width // 2)
        return remote(
            normed.at[tp, :, cols],
            far_rows.at[:, cols],
            send_x.at[half],
            recv_x.at[half],
            partner(near),
            tp,
        )

    def copy_m():
        return remote(
            places_ref.at[tp], far_places, send_x.at[2], recv_x.at[2], partner(near), tp
        )

    def copy_a(d):
        return remote(
            packs.at[d], slots.at[d, own_blk], send_a.at[d], recv_a.at[d], partner(d % near), tp
        )

    def copy_k(d):
        return remote(kv_ref, kv_all.at[me], send_k.at[d], recv_k.at[d], partner(d), tp)

    def copy_f(d):
        block = kv_all.at[partner(near)]
        return remote(block, block, send_k.at[d], recv_k.at[d], partner(d - near), tp)

    def copy_n(d):
        return remote(
            near_packs.at[d], slots.at[d, far_blk], send_y.at[d], recv_y.at[d], partner(d), tp
        )

    def copy_y(d):
        block = slots.at[d, own_blk]
        return remote(block, block, send_y.at[d], recv_y.at[d], me, row_peer)

    def copy_c(d):
        block = slots.at[d, own_blk]
        return remote(block, block, send_c.at[d], recv_c.at[d], me, pair_peer)

    def copy_b(d):
        block = slots.at[d, far_blk]
        return remote(block, block, send_b.at[d], recv_b.at[d], me, pair_peer)

    def copy_q(d):
        return remote(
            hidden_ref.at[d, other_row], hidden_in.at[d], send_q.at[d], recv_q.at[d], me, row_peer
        )

    def copy_p(d):
        return remote(
            part.at[d, other_col], pair_in.at[d], send_p.at[d], recv_p.at[d], me, pair_peer
        )

    def copy_w():
        return remote(down_hbm, down_peer, send_x.at[3], recv_x.at[3], me, row_peer)

    def copy_r(d):
        return remote(
            part.at[d, col], back.at[d], send_r.at[d], recv_r.at[d], partner(d), tp
        )

    positions = kv_ref.shape[0]
    piece_rows = positions // 4

    def copy_h(t):
        peer = (tp + t) % 4
        return remote(
            attn.at[pl.ds(pl.multiple_of(peer * piece_rows, piece_rows), piece_rows)],
            heads_all.at[tp],
            send_h.at[t],
            recv_h.at[t],
            me,
            peer,
        )

    norm_block(tp)
    pl.semaphore_wait(barrier, n + 2)
    copy_x(0).start()
    copy_x(1).start()
    copy_w().start()

    relative = jnp.bitwise_xor(routes_ref[...], me)
    route_weights = weights_ref[...]
    expert_iota = lax.broadcasted_iota(jnp.int32, (n, dev_rows), 0)
    named = []
    for b in range(4):
        span = slice(b * dev_rows, (b + 1) * dev_rows)
        hits = [relative[t : t + 1, span] == expert_iota for t in range(relative.shape[0])]
        scaled_ref[b] = functools.reduce(
            jnp.add,
            [
                jnp.where(hit, route_weights[t : t + 1, span], 0.0)
                for t, hit in enumerate(hits)
            ],
        )
        named.append(jnp.where(functools.reduce(jnp.logical_or, hits), 1.0, 0.0))
    earlier = jnp.where(
        lax.broadcasted_iota(jnp.int32, (dev_rows, dev_rows), 0)
        < lax.broadcasted_iota(jnp.int32, (dev_rows, dev_rows), 1),
        1.0,
        0.0,
    ).astype(jnp.bfloat16)
    counts = jnp.dot(
        jnp.concatenate(named, axis=0).astype(jnp.bfloat16),
        earlier,
        preferred_element_type=jnp.float32,
    )
    for b in range(4):
        places_ref[b] = jnp.where(
            named[b] > 0.5, counts[b * n : (b + 1) * n], -1.0
        ).astype(jnp.int32)
    copy_m().start()

    kv_ref[:, : key_ref.shape[1]] = key_ref[...]
    kv_ref[:, key_ref.shape[1] :] = value_ref[...]
    low = me < near

    def put_near(cols, val):
        packs[0:near, :, cols] = val.reshape(near, slot_count, val.shape[1])

    select(normed.at[tp], take(places_ref[tp], 0, near), put_near)

    @pl.loop(1, near)
    def _(d):
        copy_a(d).start()

    norm_block(row_peer)

    def put_other(cols, val):
        near_packs[:, :, cols] = val.reshape(near, slot_count, val.shape[1])

    select(normed.at[row_peer], take(places_ref[row_peer], 0, near), put_other)

    copy_n(1).start()
    fills = [
        pltpu.make_async_copy(packs.at[0], slots.at[0, own_blk], local_sem.at[4]),
        pltpu.make_async_copy(near_packs.at[0], slots.at[0, far_blk], local_sem.at[5]),
    ]
    for fill in fills:
        fill.start()

    for peer_row in range(2):
        block = peer_row * 2 + other_col
        norm_block(block)

        def put_mine(cols, val, peer_row=peer_row):
            slots[0, other_col * 2 + peer_row, :, cols] = val

        select(normed.at[block], take(places_ref[block], 0, 1), put_mine)
    for fill in fills:
        fill.wait()
    for load in loads[:3]:
        load.wait()

    def merge(j):
        for c in range(width // step):
            cols = pl.ds(c * step, step)
            part[j, col, :, cols] = (
                part[j, col, :, cols].astype(jnp.float32)
                + pair_in[j, :, cols].astype(jnp.float32)
            ).astype(part.dtype)

    def hidden_half(j, side):
        rows = slots[j, pl.ds(side * 2, 2)].reshape(2 * slot_count, width)
        gate = jnp.dot(rows, gate_ref[...], preferred_element_type=jnp.float32)
        up = jnp.dot(rows, up_ref[...], preferred_element_type=jnp.float32)
        hidden = (gate / (1.0 + jnp.exp(-gate)) * up).astype(hidden_ref.dtype)
        hidden_ref[j, 0, side] = hidden[:slot_count]
        hidden_ref[j, 1, side] = hidden[slot_count:]

    def down(j):
        units = down_ref.shape[0]
        mine = hidden_ref[j, row].reshape(2 * slot_count, units)
        other = hidden_in[j].reshape(2 * slot_count, units)
        for c in range(width // step):
            cols = pl.ds(c * step, step)
            val = jnp.dot(
                mine, down_ref[:, cols], preferred_element_type=jnp.float32
            ) + jnp.dot(other, down_peer[:, cols], preferred_element_type=jnp.float32)
            part[j, :, :, cols] = val.astype(part.dtype).reshape(2, slot_count, step)

    def spread_far():
        copy_m().wait_recv()
        taken = take(far_places[...], near, n)

        def put_far(cols, val):
            packs[near:n, :, cols] = val.reshape(n - near, slot_count, val.shape[1])
            slots[near, own_blk, :, cols] = val[:slot_count]

        for half in range(2):
            copy_x(half).wait_recv()
            chunks = width // step // 2
            select(far_rows, taken, put_far, half * chunks, (half + 1) * chunks)

        @pl.loop(near + 1, n)
        def _(d):
            copy_a(d).start()

        @pl.loop(2, near)
        def _(d):
            copy_n(d).start()

        @pl.when(low)
        def _():
            copy_k(near).start()

        @pl.loop(1, near)
        def _(d):
            @pl.when(partner(d) > me)
            def _():
                copy_k(d).start()

    def order(i):
        return jnp.where(i < 2, i, jnp.where(i < near + 2, near - 2 + i, i - near))

    def inside(j, low_bound):
        return jnp.logical_and(j >= low_bound, j < n)

    @pl.loop(0, n + 2)
    def _(i):
        d_in = order(i)
        d_mid = order(i - 1)
        d_out = order(i - 2)

        @pl.when(i == 2)
        def _():
            spread_far()

        @pl.when(inside(i, 1))
        def _():
            @pl.when(d_in != near)
            def _():
                copy_a(d_in).wait_recv()

            copy_c(d_in).start()

            @pl.when(d_in >= near)
            def _():
                copy_y(d_in).start()

        @pl.when(jnp.logical_and(i == n - 1, jnp.logical_not(low)))
        def _():
            copy_k(near).wait_recv()

            @pl.loop(near + 1, n)
            def _(d):
                copy_f(d).start()

        @pl.when(i == 2)
        def _():
            copy_w().wait_recv()

        @pl.when(inside(i - 2, 0))
        def _():
            copy_q(d_out).wait_recv()
            down(d_out)
            copy_p(d_out).start()

        @pl.when(inside(i - 2, 0))
        def _():
            copy_p(d_out).wait_recv()
            merge(d_out)

        @pl.when(inside(i - 2, 1))
        def _():
            copy_r(d_out).start()

        @pl.when(inside(i - 1, 1))
        def _():
            copy_y(d_mid).wait_recv()
            copy_b(d_mid).start()

        @pl.when(inside(i - 1, 0))
        def _():
            hidden_half(d_mid, col)

        @pl.when(inside(i - 1, 1))
        def _():
            copy_c(d_mid).wait_recv()
            copy_b(d_mid).wait_recv()

        @pl.when(inside(i - 1, 0))
        def _():
            hidden_half(d_mid, other_col)
            copy_q(d_mid).start()

    @pl.loop(1, near)
    def _(d):
        @pl.when(partner(d) < me)
        def _():
            copy_k(d).wait_recv()

    @pl.when(jnp.logical_not(low))
    def _():
        @pl.loop(near + 1, n)
        def _(d):
            copy_f(d).wait_recv()

    head_dim2 = kv_ref.shape[1] // 2
    q_heads = q_ref.shape[0] // positions
    inv_scale = (head_dim2 // 2) ** (-0.5)
    head_rows[...] = q_ref[...].astype(jnp.float32)
    map_of = lax.broadcasted_iota(jnp.int32, (positions, head_dim2), 1) // (head_dim2 // 2)
    for h in range(q_heads):
        query = head_rows[pl.ds(h, positions, stride=q_heads), :] * inv_scale
        for m in range(2):
            query_ref[2 * h + m] = jnp.where(map_of == m, query, 0.0).astype(query_ref.dtype)
    run_max[...] = jnp.full(run_max.shape, MASKED, jnp.float32)
    run_total[...] = jnp.zeros(run_total.shape, jnp.float32)
    run_acc[...] = jnp.zeros(run_acc.shape, jnp.float32)

    def visit(block, masked):
        keys = block[:, :head_dim2]
        vals = block[:, head_dim2:]
        for at in range(2 * q_heads):
            scores = lax.dot_general(
                keys, query_ref[at], (((1,), (1,)), ((), ())), preferred_element_type=jnp.float32
            )
            if masked:
                allowed = lax.broadcasted_iota(
                    jnp.int32, (positions, positions), 0
                ) <= lax.broadcasted_iota(jnp.int32, (positions, positions), 1)
                scores = jnp.where(allowed, scores, MASKED)
            old_max = run_max[at : at + 1]
            new_max = jnp.maximum(old_max, jnp.max(scores, axis=0, keepdims=True))
            shrink = jnp.exp(old_max - new_max)
            weights = jnp.exp(scores - new_max)
            run_max[at : at + 1] = new_max
            run_total[at : at + 1] = run_total[at : at + 1] * shrink + jnp.sum(
                weights, axis=0, keepdims=True
            )
            run_acc[at] = run_acc[at] * shrink + lax.dot_general(
                vals,
                weights.astype(jnp.bfloat16),
                (((0,), (0,)), ((), ())),
                preferred_element_type=jnp.float32,
            )

    visit(kv_ref, True)

    @pl.loop(0, me)
    def _(kb):
        visit(kv_all.at[kb], False)

    for h in range(q_heads):
        first = run_acc[2 * h] / run_total[2 * h : 2 * h + 1]
        second = run_acc[2 * h + 1] / run_total[2 * h + 1 : 2 * h + 2]
        head_out = jnp.transpose(first - lam_ref[h] * second)
        attn[:, h * head_dim2 : (h + 1) * head_dim2] = rms_scaled(
            head_out, head_gain_ref[...]
        ).astype(attn.dtype)

    for t in range(1, 4):
        copy_h(t).start()
    heads_all[tp] = attn[pl.ds(pl.multiple_of(tp * piece_rows, piece_rows), piece_rows), :]

    spare = jnp.zeros((dev_rows - 2 * n, dev_rows), jnp.float32)
    cols_ref[...] = jnp.transpose(
        jnp.concatenate([places_ref[tp].astype(jnp.float32), scaled_ref[tp], spare], axis=0)
    )

    def collect(first, last, rows):
        lanes = lax.broadcasted_iota(jnp.int32, cols_ref.shape, 1)
        slot = lax.broadcasted_iota(jnp.int32, (dev_rows, slot_count), 1).astype(jnp.float32)
        mixes = []
        for d in range(first, last):
            place = jnp.sum(jnp.where(lanes == d, cols_ref[...], 0.0), axis=1, keepdims=True)
            weight = jnp.sum(jnp.where(lanes == d + n, cols_ref[...], 0.0), axis=1, keepdims=True)
            mixes.append(jnp.where(slot == place, weight, 0.0))
        mix = jnp.concatenate(mixes, axis=1)
        high = mix.astype(jnp.bfloat16)
        low_part = (mix - high.astype(jnp.float32)).astype(jnp.bfloat16)
        for c in range(width // step):
            cols = pl.ds(c * step, step)
            piece = rows[..., cols].reshape((last - first) * slot_count, step)
            acc[:, cols] += jnp.dot(high, piece, preferred_element_type=jnp.float32) + jnp.dot(
                low_part, piece, preferred_element_type=jnp.float32
            )

    acc[...] = jnp.zeros(acc.shape, jnp.float32)
    collect(0, 1, part.at[0, col])

    @pl.loop(1, near)
    def _(d):
        copy_r(d).wait_recv()

    collect(1, near, back.at[1:near])

    loads[3].wait()
    for t in range(1, 4):
        copy_h(t).wait_recv()
    mixed = heads_all.shape[2]

    for c in range(width // step):
        cols = pl.ds(c * step, step)
        total = jnp.zeros((piece_rows, step), jnp.float32)
        for t in range(4):
            total = total + jnp.dot(
                heads_all[t],
                w_out_ref[t * mixed : (t + 1) * mixed, cols],
                preferred_element_type=jnp.float32,
            )
        mixer_ref[:, cols] = total.astype(mixer_ref.dtype)

    @pl.loop(near, n)
    def _(d):
        copy_r(d).wait_recv()

    collect(near, n, back.at[near:n])

    res_ref[...] = acc[...].astype(res_ref.dtype)

    @pl.when(low)
    def _():
        copy_k(near).wait_send()

    @pl.loop(1, near)
    def _(d):
        copy_n(d).wait_send()

        @pl.when(partner(d) > me)
        def _():
            copy_k(d).wait_send()

    @pl.when(jnp.logical_not(low))
    def _():
        @pl.loop(near + 1, n)
        def _(d):
            copy_f(d).wait_send()

    @pl.loop(near, n)
    def _(d):
        copy_y(d).wait_send()

    for half in range(2):
        copy_x(half).wait_send()
    copy_m().wait_send()
    copy_w().wait_send()

    @pl.loop(1, n)
    def _(d):
        @pl.when(d != near)
        def _():
            copy_a(d).wait_send()

        copy_c(d).wait_send()
        copy_b(d).wait_send()
        copy_r(d).wait_send()

    @pl.loop(0, n)
    def _(d):
        copy_p(d).wait_send()
        copy_q(d).wait_send()

    for t in range(1, 4):
        copy_h(t).wait_send()


def run_layer(n, capacity, rows, gain, routes, weights, q, keys, values, lam, head_gain, mats):
    tp_count, dev_rows, width = rows.shape
    gate_w, up_w, down_w, w_out = mats
    hidden_units = gate_w.shape[1]
    positions, head_dim2 = keys.shape
    q_heads = q.shape[0] // positions
    mixed = q_heads * head_dim2
    maps = 2 * q_heads
    dtype = rows.dtype
    near = n // 2
    vmem = pl.BlockSpec(memory_space=pltpu.VMEM)
    hbm = pl.BlockSpec(memory_space=pl.ANY)
    flops = 2 * n * 4 * capacity * width * hidden_units * 3
    return pl.pallas_call(
        functools.partial(layer_kernel, n),
        out_shape=(
            jax.ShapeDtypeStruct((positions // tp_count, width), dtype),
            jax.ShapeDtypeStruct((dev_rows, width), dtype),
        ),
        in_specs=[vmem] * 7 + [pl.BlockSpec(memory_space=pltpu.SMEM), vmem] + [hbm] * 4,
        out_specs=(vmem, vmem),
        scratch_shapes=[
            pltpu.VMEM(gate_w.shape, dtype),
            pltpu.VMEM(up_w.shape, dtype),
            pltpu.VMEM(down_w.shape, dtype),
            pltpu.VMEM(w_out.shape, dtype),
            pltpu.VMEM((tp_count, dev_rows, width), dtype),
            pltpu.VMEM((n, capacity, width), dtype),
            pltpu.VMEM((near, capacity, width), dtype),
            pltpu.VMEM((dev_rows, width), dtype),
            pltpu.VMEM((tp_count, n, dev_rows), jnp.int32),
            pltpu.VMEM((n, dev_rows), jnp.int32),
            pltpu.VMEM((tp_count, n, dev_rows), jnp.float32),
            pltpu.VMEM((dev_rows, dev_rows), jnp.float32),
            pltpu.VMEM((maps, positions, head_dim2), dtype),
            pltpu.VMEM((positions, 2 * head_dim2), dtype),
            pltpu.VMEM((n, positions, 2 * head_dim2), dtype),
            pltpu.VMEM((n, 4, capacity, width), dtype),
            pltpu.VMEM((n, 2, capacity, width), dtype),
            pltpu.VMEM((n, capacity, width), dtype),
            pltpu.VMEM((n, capacity, width), dtype),
            pltpu.VMEM((n, 2, 2, capacity, hidden_units), dtype),
            pltpu.VMEM((n, 2, capacity, hidden_units), dtype),
            pltpu.VMEM(down_w.shape, dtype),
            pltpu.VMEM((dev_rows, width), jnp.float32),
            pltpu.VMEM((maps, positions), jnp.float32),
            pltpu.VMEM((maps, positions), jnp.float32),
            pltpu.VMEM((maps, head_dim2, positions), jnp.float32),
            pltpu.VMEM(q.shape, jnp.float32),
            pltpu.VMEM((positions, mixed), dtype),
            pltpu.VMEM((tp_count, positions // tp_count, mixed), dtype),
        ]
        + [pltpu.SemaphoreType.DMA((n,))] * 16
        + [pltpu.SemaphoreType.DMA((4,))] * 4
        + [pltpu.SemaphoreType.DMA((6,))],
        compiler_params=pltpu.CompilerParams(
            collective_id=1, has_side_effects=True, vmem_limit_bytes=60 * 1024 * 1024
        ),
        cost_estimate=pl.CostEstimate(
            flops=40 * flops, bytes_accessed=16 * 1024 * 1024, transcendentals=0
        ),
    )(rows, gain, routes, weights, q, keys, values, lam, head_gain, *mats)


def one_kernel(
    queries,
    keys,
    values,
    attn_lambda,
    head_gain,
    w_out,
    moe_rows,
    moe_gain,
    routes,
    route_weights,
    w_gate,
    w_up,
    w_down,
):
    experts = lax.axis_size("ep")
    tp_count = lax.axis_size("tp")
    positions, q_heads, head_dim2 = queries.shape
    width = moe_rows.shape[1]
    dev_rows = moe_rows.shape[0] // tp_count
    capacity = 2 * dev_rows * routes.shape[1] // experts
    return run_layer(
        experts,
        capacity,
        moe_rows.reshape(tp_count, dev_rows, width),
        moe_gain.reshape(1, width),
        routes.T,
        route_weights.T,
        queries.reshape(positions * q_heads, head_dim2),
        keys.reshape(positions, head_dim2),
        values.reshape(positions, head_dim2),
        attn_lambda,
        head_gain.reshape(1, head_dim2),
        (w_gate[0], w_up[0], w_down[0], w_out),
    )


def local(
    queries,
    keys,
    values,
    attn_lambda,
    head_gain,
    w_out,
    moe_rows,
    moe_gain,
    routes,
    route_weights,
    w_gate,
    w_up,
    w_down,
):
    positions = queries.shape[0]
    q_heads = queries.shape[1]
    kv_heads = keys.shape[1]
    head_dim = queries.shape[2] // 2
    value_dim = values.shape[2]
    per_key = q_heads // kv_heads
    first_pos = lax.axis_index("ep") * positions
    query_pos = first_pos + lax.iota(jnp.int32, positions)
    last_pos = first_pos + positions - 1
    query_view = queries.reshape(positions, kv_heads, per_key, 2, head_dim)
    inv_scale = head_dim ** (-0.5)
    start_max = jnp.full((positions, kv_heads, per_key, 2), MASKED, jnp.float32)
    start_total = jnp.zeros((positions, kv_heads, per_key, 2), jnp.float32)
    start_acc = jnp.zeros((positions, kv_heads, per_key, 2, value_dim), jnp.float32)
    carry = (start_max, start_total, start_acc)
    both = jnp.concatenate([keys, values], axis=2)
    moe_out, gathered = expert_part(
        both.reshape(positions, -1),
        moe_rows,
        moe_gain,
        routes,
        route_weights,
        w_gate,
        w_up,
        w_down,
    )
    gathered = gathered.reshape(-1, kv_heads, both.shape[2])
    key_piece = gathered[:, :, : keys.shape[2]]
    value_piece = gathered[:, :, keys.shape[2] :]
    shard_count = key_piece.shape[0] // positions
    together = 1
    for candidate in (2, 3, 4):
        if shard_count % candidate == 0:
            together = candidate
    block_len = together * positions
    blocks = shard_count // together
    key_blocks = key_piece.reshape(blocks, block_len, kv_heads, 2, head_dim)
    value_blocks = value_piece.reshape(blocks, block_len, kv_heads, value_dim)
    block_starts = block_len * lax.iota(jnp.int32, blocks)

    def visit(running, inputs):
        key_blk, value_blk, block_start = inputs

        def update(current):
            run_max, run_total, run_acc = current
            key_pos = block_start + lax.iota(jnp.int32, block_len)
            scores = (
                jnp.einsum(
                    "qkgmd,pkmd->qkgmp", query_view, key_blk, preferred_element_type=jnp.float32
                )
                * inv_scale
            )
            allowed = key_pos[None, :] <= query_pos[:, None]
            scores = jnp.where(allowed[:, None, None, None, :], scores, MASKED)
            new_max = jnp.maximum(run_max, jnp.max(scores, axis=-1))
            shrink = jnp.exp(run_max - new_max)
            weights = jnp.exp(scores - new_max[..., None])
            run_total = run_total * shrink + jnp.sum(weights, axis=-1)
            run_acc = run_acc * shrink[..., None] + jnp.einsum(
                "qkgmp,pkv->qkgmv",
                weights.astype(jnp.bfloat16),
                value_blk,
                preferred_element_type=jnp.float32,
            )
            return (new_max, run_total, run_acc)

        def keep(current):
            return current

        return (lax.cond(block_start <= last_pos, update, keep, running), None)

    carry, unused = lax.scan(visit, carry, (key_blocks, value_blocks, block_starts))
    run_max, run_total, run_acc = carry
    ratios = run_acc / run_total[..., None]
    lambda_view = attn_lambda.reshape(1, kv_heads, per_key, 1)
    head_out = ratios[:, :, :, 0] - lambda_view * ratios[:, :, :, 1]
    attn_rows = (
        rms_scaled(head_out, head_gain).astype(jnp.bfloat16).reshape(positions, q_heads * value_dim)
    )
    tp_count = lax.axis_size("tp")
    tp_id = lax.axis_index("tp")
    exchanged = lax.all_to_all(
        attn_rows.reshape(positions, q_heads, value_dim),
        "tp",
        split_axis=0,
        concat_axis=1,
        tiled=True,
    )
    mixer_out = jnp.dot(
        exchanged.reshape(positions // tp_count, tp_count * q_heads * value_dim),
        w_out,
        preferred_element_type=jnp.float32,
    ).astype(jnp.bfloat16)
    return (mixer_out, moe_out)


def solution(mesh):
    experts, tp_count = mesh.shape["ep"], mesh.shape["tp"]

    def body(*args):
        keys, moe_rows, routes = args[1], args[6], args[8]
        capacity = 2 * (moe_rows.shape[0] // tp_count) * routes.shape[1] // experts
        whole_tiles = capacity % 16 == 0 and keys.shape[1] == 1
        return (one_kernel if whole_tiles else local)(*args)

    return jax.shard_map(
        body,
        mesh=mesh,
        in_specs=(
            P("ep", "tp", None),
            P("ep", "tp", None),
            P("ep", "tp", None),
            P("tp"),
            P(),
            P(),
            P("ep", None),
            P(),
            P("ep", None),
            P("ep", None),
            P("ep", None, "tp"),
            P("ep", None, "tp"),
            P("ep", "tp", None),
        ),
        out_specs=(P(("ep", "tp"), None), P(("ep", "tp"), None)),
        check_vma=False,
    )
```

```python
import functools

import jax
import jax.numpy as jnp
from jax import lax
from jax.experimental import pallas as pl
from jax.experimental.pallas import tpu as pltpu
from jax.sharding import PartitionSpec as P

EPSILON = 1e-06
MASKED = -1e30


def rms_scaled(values_f, gain):
    mean_sq = jnp.mean(values_f * values_f, axis=-1, keepdims=True)
    return values_f * lax.rsqrt(mean_sq + EPSILON) * gain


def expert_kernel(
    n,
    out_ref,
    near_ref,
    mine_ref,
    kv_ref,
    gate_ref,
    up_ref,
    down_ref,
    mix_ref,
    res_ref,
    kv_out,
    slots,
    part,
    pair_in,
    col_in,
    back,
    hidden_ref,
    acc,
    send_k,
    recv_k,
    send_a,
    recv_a,
    send_y,
    recv_y,
    send_c,
    recv_c,
    send_b,
    recv_b,
    send_p,
    recv_p,
    send_q,
    recv_q,
    send_r,
    recv_r,
    local_sem,
):
    me = lax.axis_index("ep")
    tp = lax.axis_index("tp")
    row = tp // 2
    col = tp % 2
    other_row = 1 - row
    other_col = 1 - col
    pair_peer = row * 2 + other_col
    row_peer = other_row * 2 + col
    own_blk = col * 2 + row
    far_blk = col * 2 + other_row
    slot_count = slots.shape[2]
    width = slots.shape[3]

    near = near_ref.shape[0]
    bits = [1 << b for b in range(n.bit_length() - 1)]

    def partner(d):
        total = 0
        for bit in bits:
            total = total + (me // bit + d // bit) % 2 * bit
        return total

    def remote(src, dst, ssem, rsem, ep_id, tp_id):
        return pltpu.make_async_remote_copy(
            src_ref=src,
            dst_ref=dst,
            send_sem=ssem,
            recv_sem=rsem,
            device_id=(ep_id, tp_id),
            device_id_type=pl.DeviceIdType.MESH,
        )

    barrier = pltpu.get_barrier_semaphore()

    @pl.loop(1, n)
    def _(d):
        pl.semaphore_signal(
            barrier, inc=1, device_id=(partner(d), tp), device_id_type=pl.DeviceIdType.MESH
        )

    for peer in (pair_peer, row_peer):
        pl.semaphore_signal(
            barrier, inc=1, device_id=(me, peer), device_id_type=pl.DeviceIdType.MESH
        )
    keep = pltpu.make_async_copy(kv_ref, kv_out.at[me], local_sem.at[4])
    keep.start()
    fills = [
        pltpu.make_async_copy(
            mine_ref.at[b], slots.at[0, (b % 2) * 2 + b // 2], local_sem.at[b]
        )
        for b in range(4)
    ]
    for fill in fills:
        fill.start()
    pl.semaphore_wait(barrier, n + 1)

    def copy_a(d):
        return remote(
            out_ref.at[d], slots.at[d, own_blk], send_a.at[d], recv_a.at[d], partner(d), tp
        )

    def copy_k(d):
        return remote(kv_ref, kv_out.at[me], send_k.at[d], recv_k.at[d], partner(d), tp)

    def copy_f(d):
        block = kv_out.at[partner(near)]
        return remote(block, block, send_k.at[d], recv_k.at[d], partner(d - near), tp)

    def copy_n(d):
        return remote(
            near_ref.at[d], slots.at[d, far_blk], send_y.at[d], recv_y.at[d], partner(d), tp
        )

    def copy_y(d):
        block = slots.at[d, own_blk]
        return remote(block, block, send_y.at[d], recv_y.at[d], me, row_peer)

    def copy_c(d):
        block = slots.at[d, own_blk]
        return remote(block, block, send_c.at[d], recv_c.at[d], me, pair_peer)

    def copy_b(d):
        block = slots.at[d, far_blk]
        return remote(block, block, send_b.at[d], recv_b.at[d], me, pair_peer)

    def copy_p(d):
        return remote(
            part.at[d, pl.ds(other_col * 2, 2)],
            pair_in.at[d],
            send_p.at[d],
            recv_p.at[d],
            me,
            pair_peer,
        )

    def copy_q(d):
        return remote(part.at[d, far_blk], col_in.at[d], send_q.at[d], recv_q.at[d], me, row_peer)

    def copy_r(d):
        return remote(
            part.at[d, own_blk], back.at[d], send_r.at[d], recv_r.at[d], partner(d), tp
        )

    @pl.loop(1, n)
    def _(d):
        copy_a(d).start()

        @pl.when(d < near)
        def _():
            copy_n(d).start()

    copy_k(near).start()

    @pl.loop(1, near)
    def _(d):
        copy_k(d).start()

    for fill in fills:
        fill.wait()

    def merge(index, other):
        rows = part.at[index]
        step = min(512, width)

        @pl.loop(0, width // step)
        def _(c):
            cols = pl.ds(pl.multiple_of(c * step, step), step)
            rows[:, cols] = (
                rows[:, cols].astype(jnp.float32) + other[:, cols].astype(jnp.float32)
            ).astype(part.dtype)

    def one_block(rows, put):
        gate = jnp.dot(rows, gate_ref[...], preferred_element_type=jnp.float32)
        up = jnp.dot(rows, up_ref[...], preferred_element_type=jnp.float32)
        hidden_ref[...] = (gate / (1.0 + jnp.exp(-gate)) * up).astype(hidden_ref.dtype)
        step = min(512, width)

        @pl.loop(0, width // step)
        def _(c):
            cols = pl.ds(pl.multiple_of(c * step, step), step)
            put(
                cols,
                jnp.dot(
                    hidden_ref[...], down_ref[:, cols], preferred_element_type=jnp.float32
                ).astype(part.dtype),
            )

    def compute(j):
        if slot_count % 16 == 0:

            def put(cols, val):
                part[j, :, :, cols] = val.reshape(4, slot_count, val.shape[1])

            one_block(slots[j].reshape(4 * slot_count, width), put)
        else:

            @pl.loop(0, 4)
            def _(b):
                def put(cols, val):
                    part[j, b, :, cols] = val

                one_block(slots[j, b], put)

    def inside(j, low):
        return jnp.logical_and(j >= low, j < n)

    @pl.loop(0, n + 5)
    def _(i):
        @pl.when(inside(i, 1))
        def _():
            copy_a(i).wait_recv()
            copy_c(i).start()

        @pl.when(inside(i, near))
        def _():
            copy_y(i).start()

        @pl.when(i == near)
        def _():
            copy_k(near).wait_recv()

            @pl.loop(near + 1, n)
            def _(d):
                copy_f(d).start()

        @pl.when(inside(i - 1, 1))
        def _():
            copy_y(i - 1).wait_recv()
            copy_b(i - 1).start()

        @pl.when(inside(i - 5, 0))
        def _():
            copy_q(i - 5).wait_recv()
            merge((i - 5, own_blk), col_in.at[i - 5])

        @pl.when(inside(i - 3, 0))
        def _():
            copy_p(i - 3).wait_recv()
            for y in range(2):
                merge((i - 3, col * 2 + y), pair_in.at[i - 3, y])

        @pl.when(inside(i - 2, 1))
        def _():
            copy_c(i - 2).wait_recv()
            copy_b(i - 2).wait_recv()

        @pl.when(inside(i - 2, 0))
        def _():
            compute(i - 2)

        @pl.when(inside(i - 5, 1))
        def _():
            copy_r(i - 5).start()

        @pl.when(inside(i - 3, 0))
        def _():
            copy_q(i - 3).start()

        @pl.when(inside(i - 2, 0))
        def _():
            copy_p(i - 2).start()

    def collect(d, rows):
        mix = mix_ref[d]
        high = mix.astype(jnp.bfloat16)
        low = (mix - high.astype(jnp.float32)).astype(jnp.bfloat16)
        both = jnp.dot(high, rows, preferred_element_type=jnp.float32) + jnp.dot(
            low, rows, preferred_element_type=jnp.float32
        )
        return both

    acc[...] = collect(0, part[0, own_blk])

    @pl.loop(1, n)
    def _(d):
        copy_r(d).wait_recv()
        acc[...] += collect(d, back[d])

    @pl.loop(1, near)
    def _(d):
        copy_k(d).wait()

    copy_k(near).wait_send()

    @pl.loop(near + 1, n)
    def _(d):
        copy_f(d).wait()

    keep.wait()
    res_ref[...] = acc[...].astype(res_ref.dtype)

    @pl.loop(1, n)
    def _(d):
        copy_a(d).wait_send()
        copy_y(d).wait_send()
        copy_c(d).wait_send()
        copy_b(d).wait_send()
        copy_r(d).wait_send()

    @pl.loop(0, n)
    def _(d):
        copy_p(d).wait_send()
        copy_q(d).wait_send()


def run_experts(outgoing, nearby, mine, kv, gate_w, up_w, down_w, mix):
    n, capacity, width = outgoing.shape
    hidden_units = gate_w.shape[1]
    tokens = mix.shape[1]
    rows = 4 * capacity if capacity % 16 == 0 else capacity
    dtype = outgoing.dtype
    vmem = pl.BlockSpec(memory_space=pltpu.VMEM)
    flops = 2 * n * 4 * capacity * width * hidden_units * 3
    return pl.pallas_call(
        functools.partial(expert_kernel, n),
        out_shape=(
            jax.ShapeDtypeStruct((tokens, width), dtype),
            jax.ShapeDtypeStruct((n,) + kv.shape, kv.dtype),
        ),
        in_specs=[vmem] * 8,
        out_specs=(vmem, pl.BlockSpec(memory_space=pl.ANY)),
        scratch_shapes=[
            pltpu.VMEM((n, 4, capacity, width), dtype),
            pltpu.VMEM((n, 4, capacity, width), dtype),
            pltpu.VMEM((n, 2, capacity, width), dtype),
            pltpu.VMEM((n, capacity, width), dtype),
            pltpu.VMEM((n, capacity, width), dtype),
            pltpu.VMEM((rows, hidden_units), dtype),
            pltpu.VMEM((tokens, width), jnp.float32),
        ]
        + [pltpu.SemaphoreType.DMA((n,))] * 16
        + [pltpu.SemaphoreType.DMA((5,))],
        compiler_params=pltpu.CompilerParams(
            collective_id=0, has_side_effects=True, vmem_limit_bytes=60 * 1024 * 1024
        ),
        cost_estimate=pl.CostEstimate(
            flops=40 * flops, bytes_accessed=16 * 1024 * 1024, transcendentals=0
        ),
    )(outgoing, nearby, mine, kv, gate_w, up_w, down_w, mix)


def expert_part(kv, moe_rows, moe_gain, routes, route_weights, w_gate, w_up, w_down):
    experts = lax.axis_size("ep")
    tp_count = lax.axis_size("tp")
    me = lax.axis_index("ep")
    tp_id = lax.axis_index("tp")
    dev_rows = moe_rows.shape[0] // tp_count
    top_count = routes.shape[1]
    capacity = max(2, 2 * dev_rows * top_count // experts)
    width = moe_rows.shape[1]
    normed = (
        rms_scaled(moe_rows.astype(jnp.float32), moe_gain)
        .astype(jnp.bfloat16)
        .reshape(tp_count, dev_rows, width)
    )
    relative = jnp.bitwise_xor(routes, me).reshape(tp_count, dev_rows, top_count)
    hits = relative[..., None] == lax.iota(jnp.int32, experts)
    named = jnp.any(hits, axis=2)
    before = (
        lax.iota(jnp.int32, dev_rows)[:, None] > lax.iota(jnp.int32, dev_rows)[None, :]
    ).astype(jnp.bfloat16)
    places = jnp.einsum(
        "ij,bjd->bid", before, named.astype(jnp.bfloat16), preferred_element_type=jnp.float32
    ).astype(jnp.int32)
    places = jnp.where(named, places, -1)
    slot_iota = lax.iota(jnp.int32, capacity)
    take_mine = (places[:, None, :, 0] == slot_iota[None, :, None]).astype(jnp.bfloat16)
    mine = jnp.einsum(
        "bst,btm->bsm", take_mine, normed, preferred_element_type=jnp.float32
    ).astype(jnp.bfloat16)
    own = lambda arr: lax.dynamic_index_in_dim(arr, tp_id, 0, keepdims=False)
    other_id = (1 - tp_id // 2) * 2 + tp_id % 2
    own_places = own(places)

    def fill(block, first, last):
        block_places = lax.dynamic_index_in_dim(places, block, 0, keepdims=False)[:, first:last]
        block_rows = lax.dynamic_index_in_dim(normed, block, 0, keepdims=False)
        take = (block_places.T[:, None, :] == slot_iota[None, :, None]).astype(jnp.bfloat16)
        return (
            jnp.dot(
                take.reshape(-1, dev_rows), block_rows, preferred_element_type=jnp.float32
            )
            .astype(jnp.bfloat16)
            .reshape(last - first, capacity, width)
        )

    outgoing = fill(tp_id, 0, experts)
    nearby = fill(other_id, 0, experts // 2)
    own_weights = own(route_weights.reshape(tp_count, dev_rows, top_count))
    weight_of = jnp.sum(jnp.where(own(hits), own_weights[..., None], 0.0), axis=1)
    mix = jnp.where(
        own_places.T[:, :, None] == slot_iota[None, None, :], weight_of.T[:, :, None], 0.0
    )
    return run_experts(outgoing, nearby, mine, kv, w_gate[0], w_up[0], w_down[0], mix)


def layer_kernel(
    n,
    rows_ref,
    gain_ref,
    routes_ref,
    weights_ref,
    q_ref,
    key_ref,
    value_ref,
    lam_ref,
    head_gain_ref,
    gate_hbm,
    up_hbm,
    down_hbm,
    w_out_hbm,
    mixer_ref,
    res_ref,
    gate_ref,
    up_ref,
    down_ref,
    w_out_ref,
    normed,
    packs,
    near_packs,
    far_rows,
    places_ref,
    far_places,
    scaled_ref,
    cols_ref,
    query_ref,
    kv_ref,
    kv_all,
    slots,
    part,
    pair_in,
    back,
    hidden_ref,
    hidden_in,
    down_peer,
    acc,
    run_max,
    run_total,
    run_acc,
    head_rows,
    attn,
    heads_all,
    send_k,
    recv_k,
    send_a,
    recv_a,
    send_y,
    recv_y,
    send_c,
    recv_c,
    send_b,
    recv_b,
    send_p,
    recv_p,
    send_q,
    recv_q,
    send_r,
    recv_r,
    send_h,
    recv_h,
    send_x,
    recv_x,
    send_s,
    recv_s,
    local_sem,
):
    me = lax.axis_index("ep")
    tp = lax.axis_index("tp")
    row = tp // 2
    col = tp % 2
    other_row = 1 - row
    other_col = 1 - col
    pair_peer = row * 2 + other_col
    row_peer = other_row * 2 + col
    own_blk = col * 2 + row
    far_blk = col * 2 + other_row
    slot_count = slots.shape[2]
    width = slots.shape[3]
    dev_rows = rows_ref.shape[1]
    step = min(512, width)
    near = n // 2
    bits = [1 << b for b in range(n.bit_length() - 1)]

    def partner(d):
        total = 0
        for bit in bits:
            total = total + (me // bit + d // bit) % 2 * bit
        return total

    def remote(src, dst, ssem, rsem, ep_id, tp_id):
        return pltpu.make_async_remote_copy(
            src_ref=src,
            dst_ref=dst,
            send_sem=ssem,
            recv_sem=rsem,
            device_id=(ep_id, tp_id),
            device_id_type=pl.DeviceIdType.MESH,
        )

    loads = [
        pltpu.make_async_copy(src, dst, local_sem.at[i])
        for i, (src, dst) in enumerate(
            (
                (gate_hbm, gate_ref),
                (up_hbm, up_ref),
                (down_hbm, down_ref),
                (w_out_hbm, w_out_ref),
            )
        )
    ]
    for load in loads:
        load.start()

    barrier = pltpu.get_barrier_semaphore()

    @pl.loop(1, n)
    def _(d):
        pl.semaphore_signal(
            barrier, inc=1, device_id=(partner(d), tp), device_id_type=pl.DeviceIdType.MESH
        )

    @pl.loop(1, 4)
    def _(t):
        pl.semaphore_signal(
            barrier, inc=1, device_id=(me, (tp + t) % 4), device_id_type=pl.DeviceIdType.MESH
        )

    def norm_block(b):
        @pl.loop(0, dev_rows // 16)
        def _(r):
            piece = pl.ds(pl.multiple_of(r * 16, 16), 16)
            normed[b, piece, :] = rms_scaled(
                rows_ref[b, piece, :].astype(jnp.float32), gain_ref[...]
            ).astype(normed.dtype)

    slot_iota = lax.broadcasted_iota(jnp.int32, (slot_count, dev_rows), 0)

    def take(places, first, last):
        return jnp.concatenate(
            [
                jnp.where(places[d : d + 1, :] == slot_iota, 1.0, 0.0)
                for d in range(first, last)
            ],
            axis=0,
        ).astype(jnp.bfloat16)

    def select(source, taken, put, first=0, last=width // step):
        for c in range(first, last):
            cols = pl.ds(c * step, step)
            put(
                cols,
                jnp.dot(
                    taken, source[:, cols], preferred_element_type=jnp.float32
                ).astype(packs.dtype),
            )

    def copy_x(half):
        cols = pl.ds(half * (width // 2), width // 2)
        return remote(
            normed.at[tp, :, cols],
            far_rows.at[:, cols],
            send_x.at[half],
            recv_x.at[half],
            partner(near),
            tp,
        )

    def copy_m():
        return remote(
            places_ref.at[tp], far_places, send_x.at[2], recv_x.at[2], partner(near), tp
        )

    def copy_a(d):
        return remote(
            packs.at[d], slots.at[d, own_blk], send_a.at[d], recv_a.at[d], partner(d), tp
        )

    def half_cols(half):
        return pl.ds(half * (width // 2), width // 2)

    def copy_ah(d, half):
        return remote(
            packs.at[d, :, half_cols(half)],
            slots.at[d, own_blk, :, half_cols(half)],
            send_s.at[d, half],
            recv_s.at[d, half],
            partner(d % near),
            tp,
        )

    def copy_yh(half):
        block = slots.at[near, own_blk, :, half_cols(half)]
        return remote(block, block, send_s.at[near, half], recv_s.at[near, half], me, row_peer)

    def copy_k(d):
        return remote(kv_ref, kv_all.at[me], send_k.at[d], recv_k.at[d], partner(d), tp)

    def copy_f(d):
        block = kv_all.at[partner(near)]
        return remote(block, block, send_k.at[d], recv_k.at[d], partner(d - near), tp)

    def copy_g(d):
        block = kv_all.at[partner(d - 1)]
        return remote(block, block, send_k.at[d], recv_k.at[d], partner(1), tp)

    direct = [d for d in range(1, near) if d == 1 or d % 2 == 0]
    relayed = [d for d in range(1, near) if d > 1 and d % 2]

    def copy_n(d):
        return remote(
            near_packs.at[d], slots.at[d, far_blk], send_y.at[d], recv_y.at[d], partner(d), tp
        )

    def copy_y(d):
        block = slots.at[d, own_blk]
        return remote(block, block, send_y.at[d], recv_y.at[d], me, row_peer)

    def copy_c(d):
        block = slots.at[d, own_blk]
        return remote(block, block, send_c.at[d], recv_c.at[d], me, pair_peer)

    def copy_b(d):
        block = slots.at[d, far_blk]
        return remote(block, block, send_b.at[d], recv_b.at[d], me, pair_peer)

    def copy_q(d):
        return remote(
            hidden_ref.at[d, other_row], hidden_in.at[d], send_q.at[d], recv_q.at[d], me, row_peer
        )

    def copy_p(d):
        return remote(
            part.at[d, other_col], pair_in.at[d], send_p.at[d], recv_p.at[d], me, pair_peer
        )

    def copy_w():
        return remote(down_hbm, down_peer, send_x.at[3], recv_x.at[3], me, row_peer)

    def copy_r(d):
        return remote(
            part.at[d, col], back.at[d], send_r.at[d], recv_r.at[d], partner(d), tp
        )

    positions = kv_ref.shape[0]
    piece_rows = positions // 4

    def copy_h(t):
        peer = (tp + t) % 4
        return remote(
            attn.at[pl.ds(pl.multiple_of(peer * piece_rows, piece_rows), piece_rows)],
            heads_all.at[tp],
            send_h.at[t],
            recv_h.at[t],
            me,
            peer,
        )

    norm_block(tp)
    pl.semaphore_wait(barrier, n + 2)
    copy_x(0).start()
    copy_x(1).start()
    copy_w().start()

    relative = jnp.bitwise_xor(routes_ref[...], me)
    route_weights = weights_ref[...]
    expert_iota = lax.broadcasted_iota(jnp.int32, (n, dev_rows), 0)
    named = []
    for b in range(4):
        span = slice(b * dev_rows, (b + 1) * dev_rows)
        hits = [relative[t : t + 1, span] == expert_iota for t in range(relative.shape[0])]
        scaled_ref[b] = functools.reduce(
            jnp.add,
            [
                jnp.where(hit, route_weights[t : t + 1, span], 0.0)
                for t, hit in enumerate(hits)
            ],
        )
        named.append(jnp.where(functools.reduce(jnp.logical_or, hits), 1.0, 0.0))
    earlier = jnp.where(
        lax.broadcasted_iota(jnp.int32, (dev_rows, dev_rows), 0)
        < lax.broadcasted_iota(jnp.int32, (dev_rows, dev_rows), 1),
        1.0,
        0.0,
    ).astype(jnp.bfloat16)
    counts = jnp.dot(
        jnp.concatenate(named, axis=0).astype(jnp.bfloat16),
        earlier,
        preferred_element_type=jnp.float32,
    )
    for b in range(4):
        places_ref[b] = jnp.where(
            named[b] > 0.5, counts[b * n : (b + 1) * n], -1.0
        ).astype(jnp.int32)
    copy_m().start()

    kv_ref[:, : key_ref.shape[1]] = key_ref[...]
    kv_ref[:, key_ref.shape[1] :] = value_ref[...]
    low = me < near

    def put_near(cols, val):
        packs[0:near, :, cols] = val.reshape(near, slot_count, val.shape[1])

    select(normed.at[tp], take(places_ref[tp], 0, near), put_near)

    @pl.loop(1, near)
    def _(d):
        copy_a(d).start()

    norm_block(row_peer)

    def put_other(cols, val):
        near_packs[:, :, cols] = val.reshape(3, slot_count, val.shape[1])

    select(normed.at[row_peer], take(places_ref[row_peer], 0, 3), put_other)

    copy_n(1).start()
    fills = [
        pltpu.make_async_copy(packs.at[0], slots.at[0, own_blk], local_sem.at[4]),
        pltpu.make_async_copy(near_packs.at[0], slots.at[0, far_blk], local_sem.at[5]),
    ]
    for fill in fills:
        fill.start()

    for peer_row in range(2):
        block = peer_row * 2 + other_col
        norm_block(block)

        def put_mine(cols, val, peer_row=peer_row):
            slots[0, other_col * 2 + peer_row, :, cols] = val

        select(normed.at[block], take(places_ref[block], 0, 1), put_mine)
    for fill in fills:
        fill.wait()
    for load in loads[:3]:
        load.wait()

    def merge(j):
        for c in range(width // step):
            cols = pl.ds(c * step, step)
            part[j, col, :, cols] = (
                part[j, col, :, cols].astype(jnp.float32)
                + pair_in[j, :, cols].astype(jnp.float32)
            ).astype(part.dtype)

    def hidden_half(j, side):
        rows = slots[j, pl.ds(side * 2, 2)].reshape(2 * slot_count, width)
        gate = jnp.dot(rows, gate_ref[...], preferred_element_type=jnp.float32)
        up = jnp.dot(rows, up_ref[...], preferred_element_type=jnp.float32)
        hidden = (gate / (1.0 + jnp.exp(-gate)) * up).astype(hidden_ref.dtype)
        hidden_ref[j, 0, side] = hidden[:slot_count]
        hidden_ref[j, 1, side] = hidden[slot_count:]

    def down(j):
        units = down_ref.shape[0]
        mine = hidden_ref[j, row].reshape(2 * slot_count, units)
        other = hidden_in[j].reshape(2 * slot_count, units)
        for c in range(width // step):
            cols = pl.ds(c * step, step)
            val = jnp.dot(
                mine, down_ref[:, cols], preferred_element_type=jnp.float32
            ) + jnp.dot(other, down_peer[:, cols], preferred_element_type=jnp.float32)
            part[j, :, :, cols] = val.astype(part.dtype).reshape(2, slot_count, step)

    def spread_far():
        copy_m().wait_recv()
        taken = take(far_places[...], near, n)

        def put_far(cols, val):
            packs[near:n, :, cols] = val.reshape(n - near, slot_count, val.shape[1])
            slots[near, own_blk, :, cols] = val[:slot_count]

        for half in range(2):
            copy_x(half).wait_recv()
            chunks = width // step // 2
            select(far_rows, taken, put_far, half * chunks, (half + 1) * chunks)
            if half == 0:
                copy_yh(0).start()

            @pl.loop(near + 1, n)
            def _(d):
                copy_ah(d, half).start()

        copy_n(2).start()

        @pl.when(low)
        def _():
            copy_k(near).start()

        for d in direct:

            @pl.when(partner(d) > me)
            def _(d=d):
                copy_k(d).start()

    def order(i):
        return jnp.where(i < 2, i, jnp.where(i < near + 2, near - 2 + i, i - near))

    def inside(j, low_bound):
        return jnp.logical_and(j >= low_bound, j < n)

    @pl.loop(0, n + 2)
    def _(i):
        d_in = order(i)
        d_mid = order(i - 1)
        d_out = order(i - 2)

        @pl.when(i == 2)
        def _():
            spread_far()

        @pl.when(inside(i, 1))
        def _():
            @pl.when(d_in < near)
            def _():
                copy_a(d_in).wait_recv()

            @pl.when(d_in > near)
            def _():
                for half in range(2):
                    copy_ah(d_in, half).wait_recv()

            copy_c(d_in).start()

            @pl.when(d_in == near)
            def _():
                copy_yh(1).start()

            @pl.when(jnp.logical_and(d_in >= 3, d_in != near))
            def _():
                copy_y(d_in).start()

        @pl.when(jnp.logical_and(i == n - 2, jnp.logical_not(low)))
        def _():
            copy_k(near).wait_recv()
            for d in direct:
                copy_f(near + d).start()

        @pl.when(i == n - 1)
        def _():
            for d in relayed:

                @pl.when(partner(d - 1) < me)
                def _(d=d):
                    copy_k(d - 1).wait_recv()
                    copy_g(d).start()

        @pl.when(jnp.logical_and(i == n, jnp.logical_not(low)))
        def _():
            for d in relayed:
                copy_f(near + d - 1).wait_recv()
                copy_g(near + d).start()

        @pl.when(i == 2)
        def _():
            copy_w().wait_recv()

        @pl.when(inside(i - 2, 0))
        def _():
            copy_q(d_out).wait_recv()
            down(d_out)
            copy_p(d_out).start()

        @pl.when(inside(i - 1, 1))
        def _():
            @pl.when(d_mid != near)
            def _():
                copy_y(d_mid).wait_recv()

            @pl.when(d_mid == near)
            def _():
                for half in range(2):
                    copy_yh(half).wait_recv()

            copy_b(d_mid).start()

        @pl.when(inside(i - 1, 0))
        def _():
            hidden_half(d_mid, col)

        @pl.when(inside(i - 2, 0))
        def _():
            copy_p(d_out).wait_recv()
            merge(d_out)

        @pl.when(inside(i - 2, 1))
        def _():
            copy_r(d_out).start()

        @pl.when(inside(i - 1, 1))
        def _():
            copy_c(d_mid).wait_recv()
            copy_b(d_mid).wait_recv()

        @pl.when(inside(i - 1, 0))
        def _():
            hidden_half(d_mid, other_col)
            copy_q(d_mid).start()

    waited = [d - 1 for d in relayed]
    for d in range(1, near):
        if d not in waited:

            @pl.when(partner(d) < me)
            def _(d=d):
                copy_k(d).wait_recv()

    @pl.when(jnp.logical_not(low))
    def _():
        for d in range(1, near):
            if d not in waited:
                copy_f(near + d).wait_recv()

    head_dim2 = kv_ref.shape[1] // 2
    q_heads = q_ref.shape[0] // positions
    inv_scale = (head_dim2 // 2) ** (-0.5)
    head_rows[...] = q_ref[...].astype(jnp.float32)
    map_of = lax.broadcasted_iota(jnp.int32, (positions, head_dim2), 1) // (head_dim2 // 2)
    for h in range(q_heads):
        query = head_rows[pl.ds(h, positions, stride=q_heads), :] * inv_scale
        for m in range(2):
            query_ref[2 * h + m] = jnp.where(map_of == m, query, 0.0).astype(query_ref.dtype)
    run_max[...] = jnp.full(run_max.shape, MASKED, jnp.float32)
    run_total[...] = jnp.zeros(run_total.shape, jnp.float32)
    run_acc[...] = jnp.zeros(run_acc.shape, jnp.float32)

    def visit(block, masked):
        keys = block[:, :head_dim2]
        vals = block[:, head_dim2:]
        for at in range(2 * q_heads):
            scores = lax.dot_general(
                keys, query_ref[at], (((1,), (1,)), ((), ())), preferred_element_type=jnp.float32
            )
            if masked:
                allowed = lax.broadcasted_iota(
                    jnp.int32, (positions, positions), 0
                ) <= lax.broadcasted_iota(jnp.int32, (positions, positions), 1)
                scores = jnp.where(allowed, scores, MASKED)
            old_max = run_max[at : at + 1]
            new_max = jnp.maximum(old_max, jnp.max(scores, axis=0, keepdims=True))
            shrink = jnp.exp(old_max - new_max)
            weights = jnp.exp(scores - new_max)
            run_max[at : at + 1] = new_max
            run_total[at : at + 1] = run_total[at : at + 1] * shrink + jnp.sum(
                weights, axis=0, keepdims=True
            )
            run_acc[at] = run_acc[at] * shrink + lax.dot_general(
                vals,
                weights.astype(jnp.bfloat16),
                (((0,), (0,)), ((), ())),
                preferred_element_type=jnp.float32,
            )

    visit(kv_ref, True)

    @pl.loop(0, me)
    def _(kb):
        visit(kv_all.at[kb], False)

    for h in range(q_heads):
        first = run_acc[2 * h] / run_total[2 * h : 2 * h + 1]
        second = run_acc[2 * h + 1] / run_total[2 * h + 1 : 2 * h + 2]
        head_out = jnp.transpose(first - lam_ref[h] * second)
        attn[:, h * head_dim2 : (h + 1) * head_dim2] = rms_scaled(
            head_out, head_gain_ref[...]
        ).astype(attn.dtype)

    for t in range(1, 4):
        copy_h(t).start()
    heads_all[tp] = attn[pl.ds(pl.multiple_of(tp * piece_rows, piece_rows), piece_rows), :]

    spare = jnp.zeros((dev_rows - 2 * n, dev_rows), jnp.float32)
    cols_ref[...] = jnp.transpose(
        jnp.concatenate([places_ref[tp].astype(jnp.float32), scaled_ref[tp], spare], axis=0)
    )

    def collect(first, last, rows):
        lanes = lax.broadcasted_iota(jnp.int32, cols_ref.shape, 1)
        slot = lax.broadcasted_iota(jnp.int32, (dev_rows, slot_count), 1).astype(jnp.float32)
        mixes = []
        for d in range(first, last):
            place = jnp.sum(jnp.where(lanes == d, cols_ref[...], 0.0), axis=1, keepdims=True)
            weight = jnp.sum(jnp.where(lanes == d + n, cols_ref[...], 0.0), axis=1, keepdims=True)
            mixes.append(jnp.where(slot == place, weight, 0.0))
        mix = jnp.concatenate(mixes, axis=1)
        high = mix.astype(jnp.bfloat16)
        low_part = (mix - high.astype(jnp.float32)).astype(jnp.bfloat16)
        for c in range(width // step):
            cols = pl.ds(c * step, step)
            piece = rows[..., cols].reshape((last - first) * slot_count, step)
            acc[:, cols] += jnp.dot(high, piece, preferred_element_type=jnp.float32) + jnp.dot(
                low_part, piece, preferred_element_type=jnp.float32
            )

    acc[...] = jnp.zeros(acc.shape, jnp.float32)
    collect(0, 1, part.at[0, col])

    @pl.loop(1, near)
    def _(d):
        copy_r(d).wait_recv()

    collect(1, near, back.at[1:near])

    loads[3].wait()
    for t in range(1, 4):
        copy_h(t).wait_recv()
    mixed = heads_all.shape[2]

    for c in range(width // step):
        cols = pl.ds(c * step, step)
        total = jnp.zeros((piece_rows, step), jnp.float32)
        for t in range(4):
            total = total + jnp.dot(
                heads_all[t],
                w_out_ref[t * mixed : (t + 1) * mixed, cols],
                preferred_element_type=jnp.float32,
            )
        mixer_ref[:, cols] = total.astype(mixer_ref.dtype)

    @pl.loop(near, n)
    def _(d):
        copy_r(d).wait_recv()

    collect(near, n, back.at[near:n])

    res_ref[...] = acc[...].astype(res_ref.dtype)

    @pl.when(low)
    def _():
        copy_k(near).wait_send()

    for d in direct:

        @pl.when(partner(d) > me)
        def _(d=d):
            copy_k(d).wait_send()

    for d in relayed:

        @pl.when(partner(d - 1) < me)
        def _(d=d):
            copy_g(d).wait_send()

    @pl.when(jnp.logical_not(low))
    def _():
        for d in direct:
            copy_f(near + d).wait_send()
        for d in relayed:
            copy_g(near + d).wait_send()

    for d in (1, 2):
        copy_n(d).wait_send()
    for half in range(2):
        copy_yh(half).wait_send()

    @pl.loop(3, n)
    def _(d):
        @pl.when(d != near)
        def _():
            copy_y(d).wait_send()

    for half in range(2):
        copy_x(half).wait_send()
    copy_m().wait_send()
    copy_w().wait_send()

    @pl.loop(1, n)
    def _(d):
        @pl.when(d < near)
        def _():
            copy_a(d).wait_send()

        @pl.when(d > near)
        def _():
            for half in range(2):
                copy_ah(d, half).wait_send()

        copy_c(d).wait_send()
        copy_b(d).wait_send()
        copy_r(d).wait_send()

    @pl.loop(0, n)
    def _(d):
        copy_p(d).wait_send()
        copy_q(d).wait_send()

    for t in range(1, 4):
        copy_h(t).wait_send()


def settle_kernel(mixer_in, moe_in, mixer_ref, moe_ref):
    mixer_ref[...] = mixer_in[...]
    moe_ref[...] = moe_in[...]


def run_layer(n, capacity, rows, gain, routes, weights, q, keys, values, lam, head_gain, mats):
    tp_count, dev_rows, width = rows.shape
    gate_w, up_w, down_w, w_out = mats
    hidden_units = gate_w.shape[1]
    positions, head_dim2 = keys.shape
    q_heads = q.shape[0] // positions
    mixed = q_heads * head_dim2
    maps = 2 * q_heads
    dtype = rows.dtype
    near = n // 2
    vmem = pl.BlockSpec(memory_space=pltpu.VMEM)
    hbm = pl.BlockSpec(memory_space=pl.ANY)
    flops = 2 * n * 4 * capacity * width * hidden_units * 3
    outs = pl.pallas_call(
        functools.partial(layer_kernel, n),
        out_shape=(
            jax.ShapeDtypeStruct((positions // tp_count, width), dtype),
            jax.ShapeDtypeStruct((dev_rows, width), dtype),
        ),
        in_specs=[vmem] * 7 + [pl.BlockSpec(memory_space=pltpu.SMEM), vmem] + [hbm] * 4,
        out_specs=(vmem, vmem),
        scratch_shapes=[
            pltpu.VMEM(gate_w.shape, dtype),
            pltpu.VMEM(up_w.shape, dtype),
            pltpu.VMEM(down_w.shape, dtype),
            pltpu.VMEM(w_out.shape, dtype),
            pltpu.VMEM((tp_count, dev_rows, width), dtype),
            pltpu.VMEM((n, capacity, width), dtype),
            pltpu.VMEM((3, capacity, width), dtype),
            pltpu.VMEM((dev_rows, width), dtype),
            pltpu.VMEM((tp_count, n, dev_rows), jnp.int32),
            pltpu.VMEM((n, dev_rows), jnp.int32),
            pltpu.VMEM((tp_count, n, dev_rows), jnp.float32),
            pltpu.VMEM((dev_rows, dev_rows), jnp.float32),
            pltpu.VMEM((maps, positions, head_dim2), dtype),
            pltpu.VMEM((positions, 2 * head_dim2), dtype),
            pltpu.VMEM((n, positions, 2 * head_dim2), dtype),
            pltpu.VMEM((n, 4, capacity, width), dtype),
            pltpu.VMEM((n, 2, capacity, width), dtype),
            pltpu.VMEM((n, capacity, width), dtype),
            pltpu.VMEM((n, capacity, width), dtype),
            pltpu.VMEM((n, 2, 2, capacity, hidden_units), dtype),
            pltpu.VMEM((n, 2, capacity, hidden_units), dtype),
            pltpu.VMEM(down_w.shape, dtype),
            pltpu.VMEM((dev_rows, width), jnp.float32),
            pltpu.VMEM((maps, positions), jnp.float32),
            pltpu.VMEM((maps, positions), jnp.float32),
            pltpu.VMEM((maps, head_dim2, positions), jnp.float32),
            pltpu.VMEM(q.shape, jnp.float32),
            pltpu.VMEM((positions, mixed), dtype),
            pltpu.VMEM((tp_count, positions // tp_count, mixed), dtype),
        ]
        + [pltpu.SemaphoreType.DMA((n,))] * 16
        + [pltpu.SemaphoreType.DMA((4,))] * 4
        + [pltpu.SemaphoreType.DMA((n, 2))] * 2
        + [pltpu.SemaphoreType.DMA((6,))],
        compiler_params=pltpu.CompilerParams(
            collective_id=1, has_side_effects=True, vmem_limit_bytes=60 * 1024 * 1024
        ),
        cost_estimate=pl.CostEstimate(
            flops=40 * flops, bytes_accessed=16 * 1024 * 1024, transcendentals=0
        ),
    )(rows, gain, routes, weights, q, keys, values, lam, head_gain, *mats)
    return pl.pallas_call(
        settle_kernel,
        out_shape=tuple(jax.ShapeDtypeStruct(o.shape, o.dtype) for o in outs),
        in_specs=[vmem] * 2,
        out_specs=(vmem, vmem),
    )(*outs)


def one_kernel(
    queries,
    keys,
    values,
    attn_lambda,
    head_gain,
    w_out,
    moe_rows,
    moe_gain,
    routes,
    route_weights,
    w_gate,
    w_up,
    w_down,
):
    experts = lax.axis_size("ep")
    tp_count = lax.axis_size("tp")
    positions, q_heads, head_dim2 = queries.shape
    width = moe_rows.shape[1]
    dev_rows = moe_rows.shape[0] // tp_count
    capacity = 2 * dev_rows * routes.shape[1] // experts
    return run_layer(
        experts,
        capacity,
        moe_rows.reshape(tp_count, dev_rows, width),
        moe_gain.reshape(1, width),
        routes.T,
        route_weights.T,
        queries.reshape(positions * q_heads, head_dim2),
        keys.reshape(positions, head_dim2),
        values.reshape(positions, head_dim2),
        attn_lambda,
        head_gain.reshape(1, head_dim2),
        (w_gate[0], w_up[0], w_down[0], w_out),
    )


def local(
    queries,
    keys,
    values,
    attn_lambda,
    head_gain,
    w_out,
    moe_rows,
    moe_gain,
    routes,
    route_weights,
    w_gate,
    w_up,
    w_down,
):
    positions = queries.shape[0]
    q_heads = queries.shape[1]
    kv_heads = keys.shape[1]
    head_dim = queries.shape[2] // 2
    value_dim = values.shape[2]
    per_key = q_heads // kv_heads
    first_pos = lax.axis_index("ep") * positions
    query_pos = first_pos + lax.iota(jnp.int32, positions)
    last_pos = first_pos + positions - 1
    query_view = queries.reshape(positions, kv_heads, per_key, 2, head_dim)
    inv_scale = head_dim ** (-0.5)
    start_max = jnp.full((positions, kv_heads, per_key, 2), MASKED, jnp.float32)
    start_total = jnp.zeros((positions, kv_heads, per_key, 2), jnp.float32)
    start_acc = jnp.zeros((positions, kv_heads, per_key, 2, value_dim), jnp.float32)
    carry = (start_max, start_total, start_acc)
    both = jnp.concatenate([keys, values], axis=2)
    moe_out, gathered = expert_part(
        both.reshape(positions, -1),
        moe_rows,
        moe_gain,
        routes,
        route_weights,
        w_gate,
        w_up,
        w_down,
    )
    gathered = gathered.reshape(-1, kv_heads, both.shape[2])
    key_piece = gathered[:, :, : keys.shape[2]]
    value_piece = gathered[:, :, keys.shape[2] :]
    shard_count = key_piece.shape[0] // positions
    together = 1
    for candidate in (2, 3, 4):
        if shard_count % candidate == 0:
            together = candidate
    block_len = together * positions
    blocks = shard_count // together
    key_blocks = key_piece.reshape(blocks, block_len, kv_heads, 2, head_dim)
    value_blocks = value_piece.reshape(blocks, block_len, kv_heads, value_dim)
    block_starts = block_len * lax.iota(jnp.int32, blocks)

    def visit(running, inputs):
        key_blk, value_blk, block_start = inputs

        def update(current):
            run_max, run_total, run_acc = current
            key_pos = block_start + lax.iota(jnp.int32, block_len)
            scores = (
                jnp.einsum(
                    "qkgmd,pkmd->qkgmp", query_view, key_blk, preferred_element_type=jnp.float32
                )
                * inv_scale
            )
            allowed = key_pos[None, :] <= query_pos[:, None]
            scores = jnp.where(allowed[:, None, None, None, :], scores, MASKED)
            new_max = jnp.maximum(run_max, jnp.max(scores, axis=-1))
            shrink = jnp.exp(run_max - new_max)
            weights = jnp.exp(scores - new_max[..., None])
            run_total = run_total * shrink + jnp.sum(weights, axis=-1)
            run_acc = run_acc * shrink[..., None] + jnp.einsum(
                "qkgmp,pkv->qkgmv",
                weights.astype(jnp.bfloat16),
                value_blk,
                preferred_element_type=jnp.float32,
            )
            return (new_max, run_total, run_acc)

        def keep(current):
            return current

        return (lax.cond(block_start <= last_pos, update, keep, running), None)

    carry, unused = lax.scan(visit, carry, (key_blocks, value_blocks, block_starts))
    run_max, run_total, run_acc = carry
    ratios = run_acc / run_total[..., None]
    lambda_view = attn_lambda.reshape(1, kv_heads, per_key, 1)
    head_out = ratios[:, :, :, 0] - lambda_view * ratios[:, :, :, 1]
    attn_rows = (
        rms_scaled(head_out, head_gain).astype(jnp.bfloat16).reshape(positions, q_heads * value_dim)
    )
    tp_count = lax.axis_size("tp")
    tp_id = lax.axis_index("tp")
    exchanged = lax.all_to_all(
        attn_rows.reshape(positions, q_heads, value_dim),
        "tp",
        split_axis=0,
        concat_axis=1,
        tiled=True,
    )
    mixer_out = jnp.dot(
        exchanged.reshape(positions // tp_count, tp_count * q_heads * value_dim),
        w_out,
        preferred_element_type=jnp.float32,
    ).astype(jnp.bfloat16)
    return (mixer_out, moe_out)


def solution(mesh):
    experts, tp_count = mesh.shape["ep"], mesh.shape["tp"]

    def body(*args):
        keys, moe_rows, routes = args[1], args[6], args[8]
        capacity = 2 * (moe_rows.shape[0] // tp_count) * routes.shape[1] // experts
        whole_tiles = capacity % 16 == 0 and keys.shape[1] == 1
        return (one_kernel if whole_tiles else local)(*args)

    return jax.shard_map(
        body,
        mesh=mesh,
        in_specs=(
            P("ep", "tp", None),
            P("ep", "tp", None),
            P("ep", "tp", None),
            P("tp"),
            P(),
            P(),
            P("ep", None),
            P(),
            P("ep", None),
            P("ep", None),
            P("ep", None, "tp"),
            P("ep", None, "tp"),
            P("ep", "tp", None),
        ),
        out_specs=(P(("ep", "tp"), None), P(("ep", "tp"), None)),
        check_vma=False,
    )
```

```python
import functools

import jax
import jax.numpy as jnp
from jax import lax
from jax.experimental import pallas as pl
from jax.experimental.pallas import tpu as pltpu
from jax.sharding import PartitionSpec as P

EPSILON = 1e-06
MASKED = -1e30


def rms_scaled(values_f, gain):
    mean_sq = jnp.mean(values_f * values_f, axis=-1, keepdims=True)
    return values_f * lax.rsqrt(mean_sq + EPSILON) * gain


def expert_kernel(
    n,
    out_ref,
    near_ref,
    mine_ref,
    kv_ref,
    gate_ref,
    up_ref,
    down_ref,
    mix_ref,
    res_ref,
    kv_out,
    slots,
    part,
    pair_in,
    col_in,
    back,
    hidden_ref,
    acc,
    send_k,
    recv_k,
    send_a,
    recv_a,
    send_y,
    recv_y,
    send_c,
    recv_c,
    send_b,
    recv_b,
    send_p,
    recv_p,
    send_q,
    recv_q,
    send_r,
    recv_r,
    local_sem,
):
    me = lax.axis_index("ep")
    tp = lax.axis_index("tp")
    row = tp // 2
    col = tp % 2
    other_row = 1 - row
    other_col = 1 - col
    pair_peer = row * 2 + other_col
    row_peer = other_row * 2 + col
    own_blk = col * 2 + row
    far_blk = col * 2 + other_row
    slot_count = slots.shape[2]
    width = slots.shape[3]

    near = near_ref.shape[0]
    bits = [1 << b for b in range(n.bit_length() - 1)]

    def partner(d):
        total = 0
        for bit in bits:
            total = total + (me // bit + d // bit) % 2 * bit
        return total

    def remote(src, dst, ssem, rsem, ep_id, tp_id):
        return pltpu.make_async_remote_copy(
            src_ref=src,
            dst_ref=dst,
            send_sem=ssem,
            recv_sem=rsem,
            device_id=(ep_id, tp_id),
            device_id_type=pl.DeviceIdType.MESH,
        )

    barrier = pltpu.get_barrier_semaphore()

    @pl.loop(1, n)
    def _(d):
        pl.semaphore_signal(
            barrier, inc=1, device_id=(partner(d), tp), device_id_type=pl.DeviceIdType.MESH
        )

    for peer in (pair_peer, row_peer):
        pl.semaphore_signal(
            barrier, inc=1, device_id=(me, peer), device_id_type=pl.DeviceIdType.MESH
        )
    keep = pltpu.make_async_copy(kv_ref, kv_out.at[me], local_sem.at[4])
    keep.start()
    fills = [
        pltpu.make_async_copy(
            mine_ref.at[b], slots.at[0, (b % 2) * 2 + b // 2], local_sem.at[b]
        )
        for b in range(4)
    ]
    for fill in fills:
        fill.start()
    pl.semaphore_wait(barrier, n + 1)

    def copy_a(d):
        return remote(
            out_ref.at[d], slots.at[d, own_blk], send_a.at[d], recv_a.at[d], partner(d), tp
        )

    def copy_k(d):
        return remote(kv_ref, kv_out.at[me], send_k.at[d], recv_k.at[d], partner(d), tp)

    def copy_f(d):
        block = kv_out.at[partner(near)]
        return remote(block, block, send_k.at[d], recv_k.at[d], partner(d - near), tp)

    def copy_n(d):
        return remote(
            near_ref.at[d], slots.at[d, far_blk], send_y.at[d], recv_y.at[d], partner(d), tp
        )

    def copy_y(d):
        block = slots.at[d, own_blk]
        return remote(block, block, send_y.at[d], recv_y.at[d], me, row_peer)

    def copy_c(d):
        block = slots.at[d, own_blk]
        return remote(block, block, send_c.at[d], recv_c.at[d], me, pair_peer)

    def copy_b(d):
        block = slots.at[d, far_blk]
        return remote(block, block, send_b.at[d], recv_b.at[d], me, pair_peer)

    def copy_p(d):
        return remote(
            part.at[d, pl.ds(other_col * 2, 2)],
            pair_in.at[d],
            send_p.at[d],
            recv_p.at[d],
            me,
            pair_peer,
        )

    def copy_q(d):
        return remote(part.at[d, far_blk], col_in.at[d], send_q.at[d], recv_q.at[d], me, row_peer)

    def copy_r(d):
        return remote(
            part.at[d, own_blk], back.at[d], send_r.at[d], recv_r.at[d], partner(d), tp
        )

    @pl.loop(1, n)
    def _(d):
        copy_a(d).start()

        @pl.when(d < near)
        def _():
            copy_n(d).start()

    copy_k(near).start()

    @pl.loop(1, near)
    def _(d):
        copy_k(d).start()

    for fill in fills:
        fill.wait()

    def merge(index, other):
        rows = part.at[index]
        step = min(512, width)

        @pl.loop(0, width // step)
        def _(c):
            cols = pl.ds(pl.multiple_of(c * step, step), step)
            rows[:, cols] = (
                rows[:, cols].astype(jnp.float32) + other[:, cols].astype(jnp.float32)
            ).astype(part.dtype)

    def one_block(rows, put):
        gate = jnp.dot(rows, gate_ref[...], preferred_element_type=jnp.float32)
        up = jnp.dot(rows, up_ref[...], preferred_element_type=jnp.float32)
        hidden_ref[...] = (gate / (1.0 + jnp.exp(-gate)) * up).astype(hidden_ref.dtype)
        step = min(512, width)

        @pl.loop(0, width // step)
        def _(c):
            cols = pl.ds(pl.multiple_of(c * step, step), step)
            put(
                cols,
                jnp.dot(
                    hidden_ref[...], down_ref[:, cols], preferred_element_type=jnp.float32
                ).astype(part.dtype),
            )

    def compute(j):
        if slot_count % 16 == 0:

            def put(cols, val):
                part[j, :, :, cols] = val.reshape(4, slot_count, val.shape[1])

            one_block(slots[j].reshape(4 * slot_count, width), put)
        else:

            @pl.loop(0, 4)
            def _(b):
                def put(cols, val):
                    part[j, b, :, cols] = val

                one_block(slots[j, b], put)

    def inside(j, low):
        return jnp.logical_and(j >= low, j < n)

    @pl.loop(0, n + 5)
    def _(i):
        @pl.when(inside(i, 1))
        def _():
            copy_a(i).wait_recv()
            copy_c(i).start()

        @pl.when(inside(i, near))
        def _():
            copy_y(i).start()

        @pl.when(i == near)
        def _():
            copy_k(near).wait_recv()

            @pl.loop(near + 1, n)
            def _(d):
                copy_f(d).start()

        @pl.when(inside(i - 1, 1))
        def _():
            copy_y(i - 1).wait_recv()
            copy_b(i - 1).start()

        @pl.when(inside(i - 5, 0))
        def _():
            copy_q(i - 5).wait_recv()
            merge((i - 5, own_blk), col_in.at[i - 5])

        @pl.when(inside(i - 3, 0))
        def _():
            copy_p(i - 3).wait_recv()
            for y in range(2):
                merge((i - 3, col * 2 + y), pair_in.at[i - 3, y])

        @pl.when(inside(i - 2, 1))
        def _():
            copy_c(i - 2).wait_recv()
            copy_b(i - 2).wait_recv()

        @pl.when(inside(i - 2, 0))
        def _():
            compute(i - 2)

        @pl.when(inside(i - 5, 1))
        def _():
            copy_r(i - 5).start()

        @pl.when(inside(i - 3, 0))
        def _():
            copy_q(i - 3).start()

        @pl.when(inside(i - 2, 0))
        def _():
            copy_p(i - 2).start()

    def collect(d, rows):
        mix = mix_ref[d]
        high = mix.astype(jnp.bfloat16)
        low = (mix - high.astype(jnp.float32)).astype(jnp.bfloat16)
        both = jnp.dot(high, rows, preferred_element_type=jnp.float32) + jnp.dot(
            low, rows, preferred_element_type=jnp.float32
        )
        return both

    acc[...] = collect(0, part[0, own_blk])

    @pl.loop(1, n)
    def _(d):
        copy_r(d).wait_recv()
        acc[...] += collect(d, back[d])

    @pl.loop(1, near)
    def _(d):
        copy_k(d).wait()

    copy_k(near).wait_send()

    @pl.loop(near + 1, n)
    def _(d):
        copy_f(d).wait()

    keep.wait()
    res_ref[...] = acc[...].astype(res_ref.dtype)

    @pl.loop(1, n)
    def _(d):
        copy_a(d).wait_send()
        copy_y(d).wait_send()
        copy_c(d).wait_send()
        copy_b(d).wait_send()
        copy_r(d).wait_send()

    @pl.loop(0, n)
    def _(d):
        copy_p(d).wait_send()
        copy_q(d).wait_send()


def run_experts(outgoing, nearby, mine, kv, gate_w, up_w, down_w, mix):
    n, capacity, width = outgoing.shape
    hidden_units = gate_w.shape[1]
    tokens = mix.shape[1]
    rows = 4 * capacity if capacity % 16 == 0 else capacity
    dtype = outgoing.dtype
    vmem = pl.BlockSpec(memory_space=pltpu.VMEM)
    flops = 2 * n * 4 * capacity * width * hidden_units * 3
    return pl.pallas_call(
        functools.partial(expert_kernel, n),
        out_shape=(
            jax.ShapeDtypeStruct((tokens, width), dtype),
            jax.ShapeDtypeStruct((n,) + kv.shape, kv.dtype),
        ),
        in_specs=[vmem] * 8,
        out_specs=(vmem, pl.BlockSpec(memory_space=pl.ANY)),
        scratch_shapes=[
            pltpu.VMEM((n, 4, capacity, width), dtype),
            pltpu.VMEM((n, 4, capacity, width), dtype),
            pltpu.VMEM((n, 2, capacity, width), dtype),
            pltpu.VMEM((n, capacity, width), dtype),
            pltpu.VMEM((n, capacity, width), dtype),
            pltpu.VMEM((rows, hidden_units), dtype),
            pltpu.VMEM((tokens, width), jnp.float32),
        ]
        + [pltpu.SemaphoreType.DMA((n,))] * 16
        + [pltpu.SemaphoreType.DMA((5,))],
        compiler_params=pltpu.CompilerParams(
            collective_id=0, has_side_effects=True, vmem_limit_bytes=60 * 1024 * 1024
        ),
        cost_estimate=pl.CostEstimate(
            flops=40 * flops, bytes_accessed=16 * 1024 * 1024, transcendentals=0
        ),
    )(outgoing, nearby, mine, kv, gate_w, up_w, down_w, mix)


def expert_part(kv, moe_rows, moe_gain, routes, route_weights, w_gate, w_up, w_down):
    experts = lax.axis_size("ep")
    tp_count = lax.axis_size("tp")
    me = lax.axis_index("ep")
    tp_id = lax.axis_index("tp")
    dev_rows = moe_rows.shape[0] // tp_count
    top_count = routes.shape[1]
    capacity = max(2, 2 * dev_rows * top_count // experts)
    width = moe_rows.shape[1]
    normed = (
        rms_scaled(moe_rows.astype(jnp.float32), moe_gain)
        .astype(jnp.bfloat16)
        .reshape(tp_count, dev_rows, width)
    )
    relative = jnp.bitwise_xor(routes, me).reshape(tp_count, dev_rows, top_count)
    hits = relative[..., None] == lax.iota(jnp.int32, experts)
    named = jnp.any(hits, axis=2)
    before = (
        lax.iota(jnp.int32, dev_rows)[:, None] > lax.iota(jnp.int32, dev_rows)[None, :]
    ).astype(jnp.bfloat16)
    places = jnp.einsum(
        "ij,bjd->bid", before, named.astype(jnp.bfloat16), preferred_element_type=jnp.float32
    ).astype(jnp.int32)
    places = jnp.where(named, places, -1)
    slot_iota = lax.iota(jnp.int32, capacity)
    take_mine = (places[:, None, :, 0] == slot_iota[None, :, None]).astype(jnp.bfloat16)
    mine = jnp.einsum(
        "bst,btm->bsm", take_mine, normed, preferred_element_type=jnp.float32
    ).astype(jnp.bfloat16)
    own = lambda arr: lax.dynamic_index_in_dim(arr, tp_id, 0, keepdims=False)
    other_id = (1 - tp_id // 2) * 2 + tp_id % 2
    own_places = own(places)

    def fill(block, first, last):
        block_places = lax.dynamic_index_in_dim(places, block, 0, keepdims=False)[:, first:last]
        block_rows = lax.dynamic_index_in_dim(normed, block, 0, keepdims=False)
        take = (block_places.T[:, None, :] == slot_iota[None, :, None]).astype(jnp.bfloat16)
        return (
            jnp.dot(
                take.reshape(-1, dev_rows), block_rows, preferred_element_type=jnp.float32
            )
            .astype(jnp.bfloat16)
            .reshape(last - first, capacity, width)
        )

    outgoing = fill(tp_id, 0, experts)
    nearby = fill(other_id, 0, experts // 2)
    own_weights = own(route_weights.reshape(tp_count, dev_rows, top_count))
    weight_of = jnp.sum(jnp.where(own(hits), own_weights[..., None], 0.0), axis=1)
    mix = jnp.where(
        own_places.T[:, :, None] == slot_iota[None, None, :], weight_of.T[:, :, None], 0.0
    )
    return run_experts(outgoing, nearby, mine, kv, w_gate[0], w_up[0], w_down[0], mix)


def layer_kernel(
    n,
    rows_ref,
    gain_ref,
    routes_ref,
    weights_ref,
    q_ref,
    key_ref,
    value_ref,
    lam_ref,
    head_gain_ref,
    gate_hbm,
    up_hbm,
    down_hbm,
    w_out_hbm,
    mixer_ref,
    res_ref,
    gate_ref,
    up_ref,
    down_ref,
    w_out_ref,
    normed,
    packs,
    near_packs,
    far_rows,
    places_ref,
    far_places,
    scaled_ref,
    cols_ref,
    query_ref,
    kv_ref,
    kv_all,
    slots,
    part,
    pair_in,
    back,
    hidden_ref,
    hidden_in,
    down_peer,
    acc,
    run_max,
    run_total,
    run_acc,
    head_rows,
    attn,
    heads_all,
    send_k,
    recv_k,
    send_a,
    recv_a,
    send_y,
    recv_y,
    send_c,
    recv_c,
    send_b,
    recv_b,
    send_p,
    recv_p,
    send_q,
    recv_q,
    send_r,
    recv_r,
    send_h,
    recv_h,
    send_x,
    recv_x,
    send_s,
    recv_s,
    local_sem,
):
    me = lax.axis_index("ep")
    tp = lax.axis_index("tp")
    row = tp // 2
    col = tp % 2
    other_row = 1 - row
    other_col = 1 - col
    pair_peer = row * 2 + other_col
    row_peer = other_row * 2 + col
    own_blk = col * 2 + row
    far_blk = col * 2 + other_row
    slot_count = slots.shape[2]
    width = slots.shape[3]
    dev_rows = rows_ref.shape[1]
    step = min(512, width)
    near = n // 2
    bits = [1 << b for b in range(n.bit_length() - 1)]

    def partner(d):
        total = 0
        for bit in bits:
            total = total + (me // bit + d // bit) % 2 * bit
        return total

    def remote(src, dst, ssem, rsem, ep_id, tp_id):
        return pltpu.make_async_remote_copy(
            src_ref=src,
            dst_ref=dst,
            send_sem=ssem,
            recv_sem=rsem,
            device_id=(ep_id, tp_id),
            device_id_type=pl.DeviceIdType.MESH,
        )

    loads = [
        pltpu.make_async_copy(src, dst, local_sem.at[i])
        for i, (src, dst) in enumerate(
            (
                (gate_hbm, gate_ref),
                (up_hbm, up_ref),
                (down_hbm, down_ref),
                (w_out_hbm, w_out_ref),
            )
        )
    ]
    for load in loads:
        load.start()

    barrier = pltpu.get_barrier_semaphore()

    @pl.loop(1, n)
    def _(d):
        pl.semaphore_signal(
            barrier, inc=1, device_id=(partner(d), tp), device_id_type=pl.DeviceIdType.MESH
        )

    @pl.loop(1, 4)
    def _(t):
        pl.semaphore_signal(
            barrier, inc=1, device_id=(me, (tp + t) % 4), device_id_type=pl.DeviceIdType.MESH
        )

    def norm_block(b):
        @pl.loop(0, dev_rows // 16)
        def _(r):
            piece = pl.ds(pl.multiple_of(r * 16, 16), 16)
            normed[b, piece, :] = rms_scaled(
                rows_ref[b, piece, :].astype(jnp.float32), gain_ref[...]
            ).astype(normed.dtype)

    slot_iota = lax.broadcasted_iota(jnp.int32, (slot_count, dev_rows), 0)

    def take(places, first, last):
        return jnp.concatenate(
            [
                jnp.where(places[d : d + 1, :] == slot_iota, 1.0, 0.0)
                for d in range(first, last)
            ],
            axis=0,
        ).astype(jnp.bfloat16)

    def select(source, taken, put, first=0, last=width // step):
        for c in range(first, last):
            cols = pl.ds(c * step, step)
            put(
                cols,
                jnp.dot(
                    taken, source[:, cols], preferred_element_type=jnp.float32
                ).astype(packs.dtype),
            )

    def copy_x(half):
        cols = pl.ds(half * (width // 2), width // 2)
        return remote(
            normed.at[tp, :, cols],
            far_rows.at[:, cols],
            send_x.at[half],
            recv_x.at[half],
            partner(near),
            tp,
        )

    def copy_m():
        return remote(
            places_ref.at[tp], far_places, send_x.at[2], recv_x.at[2], partner(near), tp
        )

    def copy_a(d):
        return remote(
            packs.at[d], slots.at[d, own_blk], send_a.at[d], recv_a.at[d], partner(d), tp
        )

    def half_cols(half):
        return pl.ds(half * (width // 2), width // 2)

    def copy_ah(d, half):
        return remote(
            packs.at[d, :, half_cols(half)],
            slots.at[d, own_blk, :, half_cols(half)],
            send_s.at[d, half],
            recv_s.at[d, half],
            partner(d % near),
            tp,
        )

    def copy_yh(half):
        block = slots.at[near, own_blk, :, half_cols(half)]
        return remote(block, block, send_s.at[near, half], recv_s.at[near, half], me, row_peer)

    def copy_k(d):
        return remote(kv_ref, kv_all.at[me], send_k.at[d], recv_k.at[d], partner(d), tp)

    def copy_f(d):
        block = kv_all.at[partner(near)]
        return remote(block, block, send_k.at[d], recv_k.at[d], partner(d - near), tp)

    def copy_g(d):
        block = kv_all.at[partner(d - 1)]
        return remote(block, block, send_k.at[d], recv_k.at[d], partner(1), tp)

    direct = [d for d in range(1, near) if d == 1 or d % 2 == 0]
    relayed = [d for d in range(1, near) if d > 1 and d % 2]

    def copy_n(d):
        return remote(
            near_packs.at[d], slots.at[d, far_blk], send_y.at[d], recv_y.at[d], partner(d), tp
        )

    def copy_y(d):
        block = slots.at[d, own_blk]
        return remote(block, block, send_y.at[d], recv_y.at[d], me, row_peer)

    def copy_c(d):
        block = slots.at[d, own_blk]
        return remote(block, block, send_c.at[d], recv_c.at[d], me, pair_peer)

    def copy_b(d):
        block = slots.at[d, far_blk]
        return remote(block, block, send_b.at[d], recv_b.at[d], me, pair_peer)

    def copy_q(d):
        return remote(
            hidden_ref.at[d, other_row], hidden_in.at[d], send_q.at[d], recv_q.at[d], me, row_peer
        )

    def copy_p(d):
        return remote(
            part.at[d, other_col], pair_in.at[d], send_p.at[d], recv_p.at[d], me, pair_peer
        )

    def copy_w():
        return remote(down_hbm, down_peer, send_x.at[3], recv_x.at[3], me, row_peer)

    def copy_r(d):
        return remote(
            part.at[d, col], back.at[d], send_r.at[d], recv_r.at[d], partner(d), tp
        )

    positions = kv_ref.shape[0]
    piece_rows = positions // 4

    def copy_h(t):
        peer = (tp + t) % 4
        return remote(
            attn.at[pl.ds(pl.multiple_of(peer * piece_rows, piece_rows), piece_rows)],
            heads_all.at[tp],
            send_h.at[t],
            recv_h.at[t],
            me,
            peer,
        )

    norm_block(tp)
    pl.semaphore_wait(barrier, n + 2)
    copy_x(0).start()
    copy_x(1).start()
    copy_w().start()

    relative = jnp.bitwise_xor(routes_ref[...], me)
    route_weights = weights_ref[...]
    expert_iota = lax.broadcasted_iota(jnp.int32, (n, dev_rows), 0)
    named = []
    for b in range(4):
        span = slice(b * dev_rows, (b + 1) * dev_rows)
        hits = [relative[t : t + 1, span] == expert_iota for t in range(relative.shape[0])]
        scaled_ref[b] = functools.reduce(
            jnp.add,
            [
                jnp.where(hit, route_weights[t : t + 1, span], 0.0)
                for t, hit in enumerate(hits)
            ],
        )
        named.append(jnp.where(functools.reduce(jnp.logical_or, hits), 1.0, 0.0))
    earlier = jnp.where(
        lax.broadcasted_iota(jnp.int32, (dev_rows, dev_rows), 0)
        < lax.broadcasted_iota(jnp.int32, (dev_rows, dev_rows), 1),
        1.0,
        0.0,
    ).astype(jnp.bfloat16)
    counts = jnp.dot(
        jnp.concatenate(named, axis=0).astype(jnp.bfloat16),
        earlier,
        preferred_element_type=jnp.float32,
    )
    for b in range(4):
        places_ref[b] = jnp.where(
            named[b] > 0.5, counts[b * n : (b + 1) * n], -1.0
        ).astype(jnp.int32)
    copy_m().start()

    kv_ref[:, : key_ref.shape[1]] = key_ref[...]
    kv_ref[:, key_ref.shape[1] :] = value_ref[...]
    low = me < near

    def put_near(cols, val):
        packs[0:near, :, cols] = val.reshape(near, slot_count, val.shape[1])

    select(normed.at[tp], take(places_ref[tp], 0, near), put_near)

    @pl.loop(1, near)
    def _(d):
        copy_a(d).start()

    norm_block(row_peer)

    def put_other(cols, val):
        near_packs[:, :, cols] = val.reshape(3, slot_count, val.shape[1])

    select(normed.at[row_peer], take(places_ref[row_peer], 0, 3), put_other)

    copy_n(1).start()
    copy_n(2).start()
    fills = [
        pltpu.make_async_copy(packs.at[0], slots.at[0, own_blk], local_sem.at[4]),
        pltpu.make_async_copy(near_packs.at[0], slots.at[0, far_blk], local_sem.at[5]),
    ]
    for fill in fills:
        fill.start()

    for peer_row in range(2):
        block = peer_row * 2 + other_col
        norm_block(block)

        def put_mine(cols, val, peer_row=peer_row):
            slots[0, other_col * 2 + peer_row, :, cols] = val

        select(normed.at[block], take(places_ref[block], 0, 1), put_mine)
    for fill in fills:
        fill.wait()
    for load in loads[:3]:
        load.wait()

    def merge(j):
        for c in range(width // step):
            cols = pl.ds(c * step, step)
            part[j, col, :, cols] = (
                part[j, col, :, cols].astype(jnp.float32)
                + pair_in[j, :, cols].astype(jnp.float32)
            ).astype(part.dtype)

    def hidden_half(j, side):
        rows = slots[j, pl.ds(side * 2, 2)].reshape(2 * slot_count, width)
        gate = jnp.dot(rows, gate_ref[...], preferred_element_type=jnp.float32)
        up = jnp.dot(rows, up_ref[...], preferred_element_type=jnp.float32)
        hidden = (gate / (1.0 + jnp.exp(-gate)) * up).astype(hidden_ref.dtype)
        hidden_ref[j, 0, side] = hidden[:slot_count]
        hidden_ref[j, 1, side] = hidden[slot_count:]

    def down(j):
        units = down_ref.shape[0]
        mine = hidden_ref[j, row].reshape(2 * slot_count, units)
        other = hidden_in[j].reshape(2 * slot_count, units)
        for c in range(width // step):
            cols = pl.ds(c * step, step)
            val = jnp.dot(
                mine, down_ref[:, cols], preferred_element_type=jnp.float32
            ) + jnp.dot(other, down_peer[:, cols], preferred_element_type=jnp.float32)
            part[j, :, :, cols] = val.astype(part.dtype).reshape(2, slot_count, step)

    def spread_far():
        copy_m().wait_recv()
        taken = take(far_places[...], near, n)

        def put_far(cols, val):
            packs[near:n, :, cols] = val.reshape(n - near, slot_count, val.shape[1])
            slots[near, own_blk, :, cols] = val[:slot_count]

        for half in range(2):
            copy_x(half).wait_recv()
            chunks = width // step // 2
            select(far_rows, taken, put_far, half * chunks, (half + 1) * chunks)
            if half == 0:
                copy_yh(0).start()

            @pl.loop(near + 1, n)
            def _(d):
                copy_ah(d, half).start()

        @pl.when(low)
        def _():
            copy_k(near).start()

        for d in direct:

            @pl.when(partner(d) > me)
            def _(d=d):
                copy_k(d).start()

    def order(i):
        later = jnp.where(i < near + 3, near - 3 + i, i - near)
        return jnp.where(i < 2, i, jnp.where(i < 4, near - 2 + i, jnp.where(i == 4, 2, later)))

    def inside(j, low_bound):
        return jnp.logical_and(j >= low_bound, j < n)

    @pl.loop(0, n + 2)
    def _(i):
        d_in = order(i)
        d_mid = order(i - 1)
        d_out = order(i - 2)

        @pl.when(i == 2)
        def _():
            spread_far()

        @pl.when(inside(i, 1))
        def _():
            @pl.when(d_in < near)
            def _():
                copy_a(d_in).wait_recv()

            @pl.when(d_in > near)
            def _():
                for half in range(2):
                    copy_ah(d_in, half).wait_recv()

            copy_c(d_in).start()

            @pl.when(d_in == near)
            def _():
                copy_yh(1).start()

            @pl.when(jnp.logical_and(d_in >= 3, d_in != near))
            def _():
                copy_y(d_in).start()

        @pl.when(jnp.logical_and(i == n - 2, jnp.logical_not(low)))
        def _():
            copy_k(near).wait_recv()
            for d in direct:
                copy_f(near + d).start()

        @pl.when(i == n - 1)
        def _():
            for d in relayed:

                @pl.when(partner(d - 1) < me)
                def _(d=d):
                    copy_k(d - 1).wait_recv()
                    copy_g(d).start()

        @pl.when(jnp.logical_and(i == n, jnp.logical_not(low)))
        def _():
            for d in relayed:
                copy_f(near + d - 1).wait_recv()
                copy_g(near + d).start()

        @pl.when(i == 2)
        def _():
            copy_w().wait_recv()

        @pl.when(inside(i - 2, 0))
        def _():
            copy_q(d_out).wait_recv()
            down(d_out)
            copy_p(d_out).start()

        @pl.when(inside(i - 1, 1))
        def _():
            @pl.when(d_mid != near)
            def _():
                copy_y(d_mid).wait_recv()

            @pl.when(d_mid == near)
            def _():
                for half in range(2):
                    copy_yh(half).wait_recv()

            copy_b(d_mid).start()

        @pl.when(inside(i - 1, 0))
        def _():
            hidden_half(d_mid, col)

        @pl.when(inside(i - 2, 0))
        def _():
            copy_p(d_out).wait_recv()
            merge(d_out)

        @pl.when(inside(i - 2, 1))
        def _():
            copy_r(d_out).start()

        @pl.when(inside(i - 1, 1))
        def _():
            copy_c(d_mid).wait_recv()
            copy_b(d_mid).wait_recv()

        @pl.when(inside(i - 1, 0))
        def _():
            hidden_half(d_mid, other_col)
            copy_q(d_mid).start()

    waited = [d - 1 for d in relayed]
    for d in range(1, near):
        if d not in waited:

            @pl.when(partner(d) < me)
            def _(d=d):
                copy_k(d).wait_recv()

    @pl.when(jnp.logical_not(low))
    def _():
        for d in range(1, near):
            if d not in waited:
                copy_f(near + d).wait_recv()

    head_dim2 = kv_ref.shape[1] // 2
    q_heads = q_ref.shape[0] // positions
    inv_scale = (head_dim2 // 2) ** (-0.5)
    head_rows[...] = q_ref[...].astype(jnp.float32)
    map_of = lax.broadcasted_iota(jnp.int32, (positions, head_dim2), 1) // (head_dim2 // 2)
    for h in range(q_heads):
        query = head_rows[pl.ds(h, positions, stride=q_heads), :] * inv_scale
        for m in range(2):
            query_ref[2 * h + m] = jnp.where(map_of == m, query, 0.0).astype(query_ref.dtype)
    run_max[...] = jnp.full(run_max.shape, MASKED, jnp.float32)
    run_total[...] = jnp.zeros(run_total.shape, jnp.float32)
    run_acc[...] = jnp.zeros(run_acc.shape, jnp.float32)

    def visit(block, masked):
        keys = block[:, :head_dim2]
        vals = block[:, head_dim2:]
        for at in range(2 * q_heads):
            scores = lax.dot_general(
                keys, query_ref[at], (((1,), (1,)), ((), ())), preferred_element_type=jnp.float32
            )
            if masked:
                allowed = lax.broadcasted_iota(
                    jnp.int32, (positions, positions), 0
                ) <= lax.broadcasted_iota(jnp.int32, (positions, positions), 1)
                scores = jnp.where(allowed, scores, MASKED)
            old_max = run_max[at : at + 1]
            new_max = jnp.maximum(old_max, jnp.max(scores, axis=0, keepdims=True))
            shrink = jnp.exp(old_max - new_max)
            weights = jnp.exp(scores - new_max)
            run_max[at : at + 1] = new_max
            run_total[at : at + 1] = run_total[at : at + 1] * shrink + jnp.sum(
                weights, axis=0, keepdims=True
            )
            run_acc[at] = run_acc[at] * shrink + lax.dot_general(
                vals,
                weights.astype(jnp.bfloat16),
                (((0,), (0,)), ((), ())),
                preferred_element_type=jnp.float32,
            )

    visit(kv_ref, True)

    @pl.loop(0, me)
    def _(kb):
        visit(kv_all.at[kb], False)

    for h in range(q_heads):
        first = run_acc[2 * h] / run_total[2 * h : 2 * h + 1]
        second = run_acc[2 * h + 1] / run_total[2 * h + 1 : 2 * h + 2]
        head_out = jnp.transpose(first - lam_ref[h] * second)
        attn[:, h * head_dim2 : (h + 1) * head_dim2] = rms_scaled(
            head_out, head_gain_ref[...]
        ).astype(attn.dtype)

    for t in range(1, 4):
        copy_h(t).start()
    heads_all[tp] = attn[pl.ds(pl.multiple_of(tp * piece_rows, piece_rows), piece_rows), :]

    spare = jnp.zeros((dev_rows - 2 * n, dev_rows), jnp.float32)
    cols_ref[...] = jnp.transpose(
        jnp.concatenate([places_ref[tp].astype(jnp.float32), scaled_ref[tp], spare], axis=0)
    )

    def collect(first, last, rows):
        lanes = lax.broadcasted_iota(jnp.int32, cols_ref.shape, 1)
        slot = lax.broadcasted_iota(jnp.int32, (dev_rows, slot_count), 1).astype(jnp.float32)
        mixes = []
        for d in range(first, last):
            place = jnp.sum(jnp.where(lanes == d, cols_ref[...], 0.0), axis=1, keepdims=True)
            weight = jnp.sum(jnp.where(lanes == d + n, cols_ref[...], 0.0), axis=1, keepdims=True)
            mixes.append(jnp.where(slot == place, weight, 0.0))
        mix = jnp.concatenate(mixes, axis=1)
        high = mix.astype(jnp.bfloat16)
        low_part = (mix - high.astype(jnp.float32)).astype(jnp.bfloat16)
        for c in range(width // step):
            cols = pl.ds(c * step, step)
            piece = rows[..., cols].reshape((last - first) * slot_count, step)
            acc[:, cols] += jnp.dot(high, piece, preferred_element_type=jnp.float32) + jnp.dot(
                low_part, piece, preferred_element_type=jnp.float32
            )

    acc[...] = jnp.zeros(acc.shape, jnp.float32)
    collect(0, 1, part.at[0, col])

    @pl.loop(1, near)
    def _(d):
        copy_r(d).wait_recv()

    collect(1, near, back.at[1:near])

    loads[3].wait()
    for t in range(1, 4):
        copy_h(t).wait_recv()
    mixed = heads_all.shape[2]

    for c in range(width // step):
        cols = pl.ds(c * step, step)
        total = jnp.zeros((piece_rows, step), jnp.float32)
        for t in range(4):
            total = total + jnp.dot(
                heads_all[t],
                w_out_ref[t * mixed : (t + 1) * mixed, cols],
                preferred_element_type=jnp.float32,
            )
        mixer_ref[:, cols] = total.astype(mixer_ref.dtype)

    @pl.loop(near, n)
    def _(d):
        copy_r(d).wait_recv()

    collect(near, n, back.at[near:n])

    res_ref[...] = acc[...].astype(res_ref.dtype)

    @pl.when(low)
    def _():
        copy_k(near).wait_send()

    for d in direct:

        @pl.when(partner(d) > me)
        def _(d=d):
            copy_k(d).wait_send()

    for d in relayed:

        @pl.when(partner(d - 1) < me)
        def _(d=d):
            copy_g(d).wait_send()

    @pl.when(jnp.logical_not(low))
    def _():
        for d in direct:
            copy_f(near + d).wait_send()
        for d in relayed:
            copy_g(near + d).wait_send()

    for d in (1, 2):
        copy_n(d).wait_send()
    for half in range(2):
        copy_yh(half).wait_send()

    @pl.loop(3, n)
    def _(d):
        @pl.when(d != near)
        def _():
            copy_y(d).wait_send()

    for half in range(2):
        copy_x(half).wait_send()
    copy_m().wait_send()
    copy_w().wait_send()

    @pl.loop(1, n)
    def _(d):
        @pl.when(d < near)
        def _():
            copy_a(d).wait_send()

        @pl.when(d > near)
        def _():
            for half in range(2):
                copy_ah(d, half).wait_send()

        copy_c(d).wait_send()
        copy_b(d).wait_send()
        copy_r(d).wait_send()

    @pl.loop(0, n)
    def _(d):
        copy_p(d).wait_send()
        copy_q(d).wait_send()

    for t in range(1, 4):
        copy_h(t).wait_send()


def settle_kernel(mixer_in, moe_in, mixer_ref, moe_ref):
    mixer_ref[...] = mixer_in[...]
    moe_ref[...] = moe_in[...]


def run_layer(n, capacity, rows, gain, routes, weights, q, keys, values, lam, head_gain, mats):
    tp_count, dev_rows, width = rows.shape
    gate_w, up_w, down_w, w_out = mats
    hidden_units = gate_w.shape[1]
    positions, head_dim2 = keys.shape
    q_heads = q.shape[0] // positions
    mixed = q_heads * head_dim2
    maps = 2 * q_heads
    dtype = rows.dtype
    near = n // 2
    vmem = pl.BlockSpec(memory_space=pltpu.VMEM)
    hbm = pl.BlockSpec(memory_space=pl.ANY)
    flops = 2 * n * 4 * capacity * width * hidden_units * 3
    outs = pl.pallas_call(
        functools.partial(layer_kernel, n),
        out_shape=(
            jax.ShapeDtypeStruct((positions // tp_count, width), dtype),
            jax.ShapeDtypeStruct((dev_rows, width), dtype),
        ),
        in_specs=[vmem] * 7 + [pl.BlockSpec(memory_space=pltpu.SMEM), vmem] + [hbm] * 4,
        out_specs=(vmem, vmem),
        scratch_shapes=[
            pltpu.VMEM(gate_w.shape, dtype),
            pltpu.VMEM(up_w.shape, dtype),
            pltpu.VMEM(down_w.shape, dtype),
            pltpu.VMEM(w_out.shape, dtype),
            pltpu.VMEM((tp_count, dev_rows, width), dtype),
            pltpu.VMEM((n, capacity, width), dtype),
            pltpu.VMEM((3, capacity, width), dtype),
            pltpu.VMEM((dev_rows, width), dtype),
            pltpu.VMEM((tp_count, n, dev_rows), jnp.int32),
            pltpu.VMEM((n, dev_rows), jnp.int32),
            pltpu.VMEM((tp_count, n, dev_rows), jnp.float32),
            pltpu.VMEM((dev_rows, dev_rows), jnp.float32),
            pltpu.VMEM((maps, positions, head_dim2), dtype),
            pltpu.VMEM((positions, 2 * head_dim2), dtype),
            pltpu.VMEM((n, positions, 2 * head_dim2), dtype),
            pltpu.VMEM((n, 4, capacity, width), dtype),
            pltpu.VMEM((n, 2, capacity, width), dtype),
            pltpu.VMEM((n, capacity, width), dtype),
            pltpu.VMEM((n, capacity, width), dtype),
            pltpu.VMEM((n, 2, 2, capacity, hidden_units), dtype),
            pltpu.VMEM((n, 2, capacity, hidden_units), dtype),
            pltpu.VMEM(down_w.shape, dtype),
            pltpu.VMEM((dev_rows, width), jnp.float32),
            pltpu.VMEM((maps, positions), jnp.float32),
            pltpu.VMEM((maps, positions), jnp.float32),
            pltpu.VMEM((maps, head_dim2, positions), jnp.float32),
            pltpu.VMEM(q.shape, jnp.float32),
            pltpu.VMEM((positions, mixed), dtype),
            pltpu.VMEM((tp_count, positions // tp_count, mixed), dtype),
        ]
        + [pltpu.SemaphoreType.DMA((n,))] * 16
        + [pltpu.SemaphoreType.DMA((4,))] * 4
        + [pltpu.SemaphoreType.DMA((n, 2))] * 2
        + [pltpu.SemaphoreType.DMA((6,))],
        compiler_params=pltpu.CompilerParams(
            collective_id=1, has_side_effects=True, vmem_limit_bytes=60 * 1024 * 1024
        ),
        cost_estimate=pl.CostEstimate(
            flops=40 * flops, bytes_accessed=16 * 1024 * 1024, transcendentals=0
        ),
    )(rows, gain, routes, weights, q, keys, values, lam, head_gain, *mats)
    return pl.pallas_call(
        settle_kernel,
        out_shape=tuple(jax.ShapeDtypeStruct(o.shape, o.dtype) for o in outs),
        in_specs=[vmem] * 2,
        out_specs=(vmem, vmem),
    )(*outs)


def one_kernel(
    queries,
    keys,
    values,
    attn_lambda,
    head_gain,
    w_out,
    moe_rows,
    moe_gain,
    routes,
    route_weights,
    w_gate,
    w_up,
    w_down,
):
    experts = lax.axis_size("ep")
    tp_count = lax.axis_size("tp")
    positions, q_heads, head_dim2 = queries.shape
    width = moe_rows.shape[1]
    dev_rows = moe_rows.shape[0] // tp_count
    capacity = 2 * dev_rows * routes.shape[1] // experts
    return run_layer(
        experts,
        capacity,
        moe_rows.reshape(tp_count, dev_rows, width),
        moe_gain.reshape(1, width),
        routes.T,
        route_weights.T,
        queries.reshape(positions * q_heads, head_dim2),
        keys.reshape(positions, head_dim2),
        values.reshape(positions, head_dim2),
        attn_lambda,
        head_gain.reshape(1, head_dim2),
        (w_gate[0], w_up[0], w_down[0], w_out),
    )


def local(
    queries,
    keys,
    values,
    attn_lambda,
    head_gain,
    w_out,
    moe_rows,
    moe_gain,
    routes,
    route_weights,
    w_gate,
    w_up,
    w_down,
):
    positions = queries.shape[0]
    q_heads = queries.shape[1]
    kv_heads = keys.shape[1]
    head_dim = queries.shape[2] // 2
    value_dim = values.shape[2]
    per_key = q_heads // kv_heads
    first_pos = lax.axis_index("ep") * positions
    query_pos = first_pos + lax.iota(jnp.int32, positions)
    last_pos = first_pos + positions - 1
    query_view = queries.reshape(positions, kv_heads, per_key, 2, head_dim)
    inv_scale = head_dim ** (-0.5)
    start_max = jnp.full((positions, kv_heads, per_key, 2), MASKED, jnp.float32)
    start_total = jnp.zeros((positions, kv_heads, per_key, 2), jnp.float32)
    start_acc = jnp.zeros((positions, kv_heads, per_key, 2, value_dim), jnp.float32)
    carry = (start_max, start_total, start_acc)
    both = jnp.concatenate([keys, values], axis=2)
    moe_out, gathered = expert_part(
        both.reshape(positions, -1),
        moe_rows,
        moe_gain,
        routes,
        route_weights,
        w_gate,
        w_up,
        w_down,
    )
    gathered = gathered.reshape(-1, kv_heads, both.shape[2])
    key_piece = gathered[:, :, : keys.shape[2]]
    value_piece = gathered[:, :, keys.shape[2] :]
    shard_count = key_piece.shape[0] // positions
    together = 1
    for candidate in (2, 3, 4):
        if shard_count % candidate == 0:
            together = candidate
    block_len = together * positions
    blocks = shard_count // together
    key_blocks = key_piece.reshape(blocks, block_len, kv_heads, 2, head_dim)
    value_blocks = value_piece.reshape(blocks, block_len, kv_heads, value_dim)
    block_starts = block_len * lax.iota(jnp.int32, blocks)

    def visit(running, inputs):
        key_blk, value_blk, block_start = inputs

        def update(current):
            run_max, run_total, run_acc = current
            key_pos = block_start + lax.iota(jnp.int32, block_len)
            scores = (
                jnp.einsum(
                    "qkgmd,pkmd->qkgmp", query_view, key_blk, preferred_element_type=jnp.float32
                )
                * inv_scale
            )
            allowed = key_pos[None, :] <= query_pos[:, None]
            scores = jnp.where(allowed[:, None, None, None, :], scores, MASKED)
            new_max = jnp.maximum(run_max, jnp.max(scores, axis=-1))
            shrink = jnp.exp(run_max - new_max)
            weights = jnp.exp(scores - new_max[..., None])
            run_total = run_total * shrink + jnp.sum(weights, axis=-1)
            run_acc = run_acc * shrink[..., None] + jnp.einsum(
                "qkgmp,pkv->qkgmv",
                weights.astype(jnp.bfloat16),
                value_blk,
                preferred_element_type=jnp.float32,
            )
            return (new_max, run_total, run_acc)

        def keep(current):
            return current

        return (lax.cond(block_start <= last_pos, update, keep, running), None)

    carry, unused = lax.scan(visit, carry, (key_blocks, value_blocks, block_starts))
    run_max, run_total, run_acc = carry
    ratios = run_acc / run_total[..., None]
    lambda_view = attn_lambda.reshape(1, kv_heads, per_key, 1)
    head_out = ratios[:, :, :, 0] - lambda_view * ratios[:, :, :, 1]
    attn_rows = (
        rms_scaled(head_out, head_gain).astype(jnp.bfloat16).reshape(positions, q_heads * value_dim)
    )
    tp_count = lax.axis_size("tp")
    tp_id = lax.axis_index("tp")
    exchanged = lax.all_to_all(
        attn_rows.reshape(positions, q_heads, value_dim),
        "tp",
        split_axis=0,
        concat_axis=1,
        tiled=True,
    )
    mixer_out = jnp.dot(
        exchanged.reshape(positions // tp_count, tp_count * q_heads * value_dim),
        w_out,
        preferred_element_type=jnp.float32,
    ).astype(jnp.bfloat16)
    return (mixer_out, moe_out)


def solution(mesh):
    experts, tp_count = mesh.shape["ep"], mesh.shape["tp"]

    def body(*args):
        keys, moe_rows, routes = args[1], args[6], args[8]
        capacity = 2 * (moe_rows.shape[0] // tp_count) * routes.shape[1] // experts
        whole_tiles = capacity % 16 == 0 and keys.shape[1] == 1 and experts >= 8
        return (one_kernel if whole_tiles else local)(*args)

    return jax.shard_map(
        body,
        mesh=mesh,
        in_specs=(
            P("ep", "tp", None),
            P("ep", "tp", None),
            P("ep", "tp", None),
            P("tp"),
            P(),
            P(),
            P("ep", None),
            P(),
            P("ep", None),
            P("ep", None),
            P("ep", None, "tp"),
            P("ep", None, "tp"),
            P("ep", "tp", None),
        ),
        out_specs=(P(("ep", "tp"), None), P(("ep", "tp"), None)),
        check_vma=False,
    )
```
